512 devices in a mesh: ep: 32 (over z, x), tp: 16 (over y, core).
Axes of the slice: x: 4, y: 8, z: 8, core: 2. Of those that a mesh axis runs over, the one named last changes fastest.
Arguments:
- conv_value: bfloat16 [16384, 2048], P('ep', 'tp'), may hold values from -6 to 6
- conv_gate: bfloat16 [16384, 2048], P('ep', 'tp'), may hold values from -9 to 9
- conv_taps: float32 [31, 2048], P(None, 'tp'), may hold values from -14 to 14
- norm_gain: float32 [2048], P('tp'), may hold values from 0.1 to 1.9
- norm_shift: float32 [2048], P('tp'), may hold values from -3 to 3
- conv_out_weight: bfloat16 [2048, 2048], P(None, 'tp'), may hold values from -0.125 to 0.125
- moe_input: bfloat16 [4096, 2048], P('ep'), may hold values from -6 to 6
- moe_gain: float32 [2048], replicated, may hold values from 0.1 to 1.9
- routes: int32 [4096, 4], P('ep'), may hold values from 0 to 31, all different within a row; in each aligned block of 128 rows (0 to 127, 128 to 255, ...) at most 32 rows name the same one
- route_weights: float32 [4096, 4], P('ep'), may hold values from 0.25 to 1
- expert_gate: bfloat16 [32, 2048, 4096], P('ep', None, 'tp'), may hold values from -0.125 to 0.125
- expert_up: bfloat16 [32, 2048, 4096], P('ep', None, 'tp'), may hold values from -0.125 to 0.125
- expert_down: bfloat16 [32, 4096, 2048], P('ep', None, 'tp'), may hold values from -0.09375 to 0.09375
- shared_gate: bfloat16 [2048, 512], P(None, 'tp'), may hold values from -0.125 to 0.125
- shared_up: bfloat16 [2048, 512], P(None, 'tp'), may hold values from -0.125 to 0.125
- shared_down: bfloat16 [512, 2048], P(None, 'tp'), may hold values from -0.25 to 0.25
Outputs:
- conv_result: bfloat16 [16384, 2048], P('ep', 'tp')
- moe_result: bfloat16 [4096, 2048], P('ep', 'tp')
The draws below stay inside these ranges and needn't reach their ends.
Inputs may be any that keep to these rules, and one draw needn't show every extreme that they name: `routes`: in the rows of one device (aligned blocks of 128 rows) no expert is named by more than 32 rows, a bound that some block reaches; each row names 4 different experts.
All inputs are finite; a program needn't handle non-finite values.
Results may differ from the reference program's by a relative error of at most 0.0068.
Values may be sent and summed in bfloat16 or wider, within the bound.
A program may use at most 64 MiB of HBM per device.

```python
import math
import jax
import jax.numpy as jnp
import numpy as np
from jax import lax

D = 2048
FF = 4096
SHARED_FF = 512
CONV_WIDTH = 31
TOPK = 4
TOKB_DEV = 128
TOK_A = 16384
TOK_B = 4096
EXPERTS = 32
CAP = 32
N_EP = 32


def draw_conv_taps(key, part):
    base_key = jax.random.fold_in(key, 11)
    rough_key = jax.random.fold_in(key, 12)
    channel = jnp.arange(D, dtype=jnp.float32) / D
    base_draw = jnp.clip(jax.random.normal(base_key, (CONV_WIDTH, D), jnp.float32), -5.0, 5.0)
    channel_rise = jnp.exp(jnp.log(4.0) * channel)
    rough_scale = jax.random.uniform(rough_key, (D,), jnp.float32, 0.5, 1.5)
    return base_draw * channel_rise * rough_scale / jnp.sqrt(CONV_WIDTH * 1.0)


def block_scale(stream_key, shape, split, least, high):
    factor_of = 1.0
    for dim, blocks in split:
        draws = jax.random.uniform(jax.random.fold_in(jax.random.fold_in(stream_key, 6), dim), (blocks,), jnp.float32, least / len(split), high / len(split))
        factor_of = factor_of * jnp.repeat(jnp.exp(draws), shape[dim] // blocks).reshape((-1,) + (1,) * (len(shape) - 1 - dim))
    return factor_of


def routed_block(stream_key, own, number, rows, number_of, top, most, skew):
    order = jax.random.permutation(stream_key, number_of)
    packed, common = shares(number_of, rows * top, most, skew, True), shares(number_of, rows * top, most, skew, False)
    places = jnp.arange(number_of)

    def named(sizes, rotation):
        used = int((sizes > 0).sum())
        fixed = max(1, used // 4)
        shifted = fixed + (places - fixed + rotation * (used - fixed)) % max(1, number_of - fixed)
        return jnp.zeros((number_of,), jnp.int32).at[order[jnp.where(places < fixed, places, shifted)]].set(jnp.asarray(sizes, jnp.int32))

    sizes = jnp.where(number % 4 == 0, named(packed, number // 4), named(common, number - number // 4 - 1))
    mixed = jax.random.permutation(jax.random.fold_in(own, 3), number_of)
    giver, receiver = mixed[0:number_of // 2 * 2:2], mixed[1:number_of // 2 * 2:2]
    slack = jnp.minimum(sizes[giver] - 1, most - sizes[receiver]) // 2
    slack = jnp.where((giver == order[0]) | (receiver == order[0]) | (sizes[receiver] == 0), 0, jnp.maximum(slack, 0))
    shifted = jax.random.randint(jax.random.fold_in(own, 4), (number_of // 2,), 0, 1 << 20) % (slack + 1)
    sizes = sizes.at[giver].add(-shifted).at[receiver].add(shifted)
    items = jnp.searchsorted(jnp.cumsum(sizes), jnp.arange(rows * top), side="right").astype(jnp.int32)
    listing = items.reshape(top, rows).T
    listing = listing[jax.random.permutation(jax.random.fold_in(own, 1), rows)]
    rotation = jax.random.randint(jax.random.fold_in(own, 2), (rows, 1), 0, top)
    return jnp.take_along_axis(listing, (jnp.arange(top)[None, :] + rotation) % top, axis=1)


def shares(amount, total, reach, skew, full):
    portions = [(1 << 20) // math.isqrt(rank ** skew) + 1 for rank in range(1, amount + 1)]
    largest = reach if full else min(reach, max(-(-total // amount), total * portions[0] // sum(portions)))
    least = 1 if total - largest >= amount - 1 else 0
    given, surplus = [largest] + [least] * (amount - 1), total - largest - least * (amount - 1)
    while surplus > 0:
        movable = [i for i in range(1, amount) if given[i] < largest] or [i for i in range(1, amount) if given[i] < reach]
        whole, left = sum([portions[i] for i in movable]), surplus
        for i in movable:
            extra = min(reach - given[i], max(1, left * portions[i] // whole), surplus)
            given[i] = given[i] + extra
            surplus = surplus - extra
    return np.array(given)


def noise(rng, shape, width, reach, shards=(), kind=jnp.bfloat16):
    array = jax.random.normal(rng, shape, jnp.float32) * width
    if len(shards) > 0:
        array = block_scale(rng, shape, shards, -0.22, 0.18) * array
    return jnp.clip(array, min=-reach, max=reach).astype(kind)


def setup_inputs(seed: int = 0) -> dict:
    key_list = jax.random.split(jax.random.key(seed), 17)
    conv_value = noise(key_list[0], (TOK_A, D), 1.0, 6.0, ((0, 32), (1, 16)))
    conv_gate = noise(key_list[1], (TOK_A, D), 1.5, 9.0, ((0, 32), (1, 16)))
    conv_taps = draw_conv_taps(jax.random.fold_in(key_list[16], 71), 0)
    norm_gain = jnp.clip(1.0 + 0.18 * jax.random.normal(key_list[3], (D,), jnp.float32), 0.1, 1.9)
    norm_shift = noise(key_list[4], (D,), 0.5, 3.0, ((0, 16),), jnp.float32)
    conv_out_weight = noise(key_list[5], (D, D), D ** -0.5, 0.125, ((1, 16),))
    moe_input = noise(key_list[6], (TOK_B, D), 1.0, 6.0, ((0, 32),))
    moe_gain = jnp.clip(1.0 + 0.18 * jax.random.normal(key_list[7], (D,), jnp.float32), 0.1, 1.9)
    routes_keys = jax.random.split(jax.random.fold_in(key_list[8], 1), TOK_B // TOKB_DEV)
    routes_turns = jax.random.permutation(jax.random.fold_in(key_list[8], 3), TOK_B // TOKB_DEV)
    routes = jax.vmap(lambda own, number: routed_block(jax.random.fold_in(key_list[8], 2), own, number, TOKB_DEV, EXPERTS, TOPK, CAP, 2))(routes_keys, routes_turns).reshape((TOK_B, TOPK))
    route_weights = jnp.clip(0.25 + 0.75 * jax.random.uniform(key_list[9], (TOK_B, TOPK), jnp.float32) ** block_scale(key_list[9], (TOK_B, TOPK), ((0, 32),), -0.2, 0.2), 0.25, 1.0)
    expert_gate = noise(key_list[10], (EXPERTS, D, FF), D ** -0.5, 0.125, ((0, 32), (2, 16)))
    expert_up = noise(key_list[11], (EXPERTS, D, FF), D ** -0.5, 0.125, ((0, 32), (2, 16)))
    expert_down = noise(key_list[12], (EXPERTS, FF, D), FF ** -0.5, 0.09375, ((0, 32), (2, 16)))
    shared_gate = noise(key_list[13], (D, SHARED_FF), D ** -0.5, 0.125, ((1, 16),))
    shared_up = noise(key_list[14], (D, SHARED_FF), D ** -0.5, 0.125, ((1, 16),))
    shared_down = noise(key_list[15], (SHARED_FF, D), SHARED_FF ** -0.5, 0.25, ((1, 16),))
    return {"conv_value": conv_value, "conv_gate": conv_gate, "conv_taps": conv_taps, "norm_gain": norm_gain, "norm_shift": norm_shift, "conv_out_weight": conv_out_weight, "moe_input": moe_input, "moe_gain": moe_gain, "routes": routes, "route_weights": route_weights, "expert_gate": expert_gate, "expert_up": expert_up, "expert_down": expert_down, "shared_gate": shared_gate, "shared_up": shared_up, "shared_down": shared_down}


def reference(conv_value, conv_gate, conv_taps, norm_gain, norm_shift, conv_out_weight, moe_input, moe_gain, routes, route_weights, expert_gate, expert_up, expert_down, shared_gate, shared_up, shared_down):
    glu_rows = (conv_value.astype(jnp.float32) * jax.nn.sigmoid(conv_gate.astype(jnp.float32))).astype(jnp.bfloat16)
    padded = jnp.concatenate([jnp.zeros((CONV_WIDTH - 1, D), jnp.bfloat16), glu_rows], axis=0)
    filtered = jnp.zeros((TOK_A, D), jnp.float32)
    for offset in range(CONV_WIDTH):
        filtered = filtered + conv_taps[offset] * padded[offset:offset + TOK_A].astype(jnp.float32)
    row_mean = lax.optimization_barrier(jnp.mean(filtered, axis=1, keepdims=True))
    row_square = lax.optimization_barrier(jnp.mean(filtered * filtered, axis=1, keepdims=True))
    scaled = (filtered - row_mean) * lax.rsqrt(row_square - row_mean * row_mean + 1e-05)
    conv_hidden = jax.nn.silu(scaled * norm_gain + norm_shift).astype(jnp.bfloat16)
    conv_result = jnp.dot(conv_hidden, conv_out_weight, preferred_element_type=jnp.float32).astype(jnp.bfloat16)
    inputs = moe_input.astype(jnp.float32)
    normed = (inputs * lax.rsqrt(lax.optimization_barrier(jnp.mean(inputs * inputs, axis=1, keepdims=True)) + 1e-06) * moe_gain).astype(jnp.bfloat16)
    flat_expert = routes.reshape(-1).astype(jnp.int32)
    owner_row = (jnp.arange(TOK_B * TOPK, dtype=jnp.int32) // TOPK).astype(jnp.int32)
    sort_order = jnp.argsort(flat_expert, stable=True).astype(jnp.int32)
    sorted_owner = owner_row[sort_order]
    sorted_weight = route_weights.reshape(-1)[sort_order]
    counts = lax.optimization_barrier(jnp.sum((flat_expert[:, None] == jnp.arange(EXPERTS, dtype=jnp.int32)[None, :]).astype(jnp.int32), axis=0))
    starts = (jnp.cumsum(counts) - counts).astype(jnp.int32)
    slot_limit = N_EP * CAP
    pad_owner = jnp.concatenate([sorted_owner, jnp.zeros((slot_limit,), jnp.int32)])
    pad_weight = jnp.concatenate([sorted_weight, jnp.zeros((slot_limit,), jnp.float32)])

    def one_expert(running, expert_id):
        first_row = starts[expert_id]
        row_ids = lax.dynamic_slice_in_dim(pad_owner, first_row, slot_limit)
        weight = lax.dynamic_slice_in_dim(pad_weight, first_row, slot_limit)
        live_mask = (jnp.arange(slot_limit, dtype=jnp.int32) < counts[expert_id]).astype(jnp.float32)
        picked_rows = normed[row_ids]
        hidden = (jax.nn.silu(jnp.dot(picked_rows, expert_gate[expert_id], preferred_element_type=jnp.float32)) * jnp.dot(picked_rows, expert_up[expert_id], preferred_element_type=jnp.float32)).astype(jnp.bfloat16)
        expert_rows = jnp.dot(hidden, expert_down[expert_id], preferred_element_type=jnp.float32).astype(jnp.bfloat16)
        expert_rows = lax.optimization_barrier(expert_rows).astype(jnp.float32)
        return (running.at[row_ids].add(expert_rows * (weight * live_mask)[:, None]), None)
    routed, _ = lax.scan(one_expert, jnp.zeros((TOK_B, D), jnp.float32), jnp.arange(EXPERTS, dtype=jnp.int32))
    shared_hidden = (jax.nn.silu(jnp.dot(normed, shared_gate, preferred_element_type=jnp.float32)) * jnp.dot(normed, shared_up, preferred_element_type=jnp.float32)).astype(jnp.bfloat16)
    shared_sum = jnp.dot(shared_hidden, shared_down, preferred_element_type=jnp.float32)
    moe_result = (routed + shared_sum).astype(jnp.bfloat16)
    return (conv_result, moe_result)
```

```python
import functools

import jax
import jax.numpy as jnp
from jax import lax
from jax.experimental import pallas as pl
from jax.experimental.pallas import tpu as pltpu
from jax.sharding import PartitionSpec as P

MESH = pl.DeviceIdType.MESH
F32 = jnp.float32
BF16 = jnp.bfloat16

NZ, NX, NY, NC = 8, 4, 8, 2
N_EP, N_TP = NZ * NX, NY * NC
D = 2048
CH = D // N_TP
TAPS = 31
HALO = 32
ROWS_A = 512
TOK = 128
CAP = 32
SLOTS = N_EP * CAP
TOPK = 4
HID = 256
SH = 32
GROUPS = 4
GROWS = SLOTS // GROUPS
CBROWS = ROWS_A + SH


def dot(a, b, dims=(((1,), (0,)), ((), ())), precision=None):
    return lax.dot_general(a, b, dims, precision=precision, preferred_element_type=F32)


NT = (((1,), (1,)), ((), ()))
TN = (((0,), (0,)), ((), ()))


def sigmoid(v):
    return 1.0 / (1.0 + jnp.exp(-v))


def silu(v):
    return v / (1.0 + jnp.exp(-v))


class Ring:
    def __init__(self, place, piece, half, sems, here):
        self.piece, self.half, self.here = piece, half, here
        self.sr, self.sl, self.rr, self.rl, self.ps, self.pr = (s.at[place] for s in sems)
        self.sent = []

    def chip(self, d):
        return lax.rem(self.here["y"] + d + 2 * NY, NY)

    def start(self, ref, send, recv, to):
        copy = pltpu.make_async_remote_copy(
            src_ref=ref, dst_ref=ref, send_sem=send, recv_sem=recv,
            device_id=(self.here["ep"], to), device_id_type=MESH,
        )
        copy.start()
        self.sent.append(copy)

    def wait_at(self, ref, send, recv, frm):
        pltpu.make_async_remote_copy(
            src_ref=ref, dst_ref=ref, send_sem=send, recv_sem=recv,
            device_id=(self.here["ep"], frm), device_id_type=MESH,
        ).wait_recv()

    def at(self, chip, core, part=None):
        t = chip * NC + core
        return self.piece(t) if part is None else self.half(t, part)

    def own(self):
        h = self.here
        mine = self.at(h["y"], h["core"])
        self.start(mine, self.sr.at[0], self.rr.at[0], h["right"])
        self.start(mine, self.sl.at[0], self.rl.at[0], h["left"])
        self.start(mine, self.ps.at[0], self.pr.at[0], h["partner"])

    def stage(self, d):
        h = self.here
        for way, (ss, rs, sign, to, frm) in enumerate(
            ((self.sr, self.rr, -1, h["right"], h["left"]), (self.sl, self.rl, 1, h["left"], h["right"]))
        ):
            chip = self.chip(sign * d)
            got = self.at(chip, h["core"], way if d == 4 else None)
            self.wait_at(got, ss.at[d - 1], rs.at[d - 1], frm)
            if d < 3:
                self.start(got, ss.at[d], rs.at[d], to)
            elif d == 3:
                self.start(self.at(chip, h["core"], way), ss.at[3], rs.at[3], to)
            k = 1 + way * 4 + (d - 1)
            self.start(got, self.ps.at[k], self.pr.at[k], h["partner"])

    def from_partner(self, d):
        h = self.here
        if d == 0:
            self.wait_at(self.at(h["y"], 1 - h["core"]), self.ps.at[0], self.pr.at[0], h["partner"])
            return
        for way, sign in enumerate((-1, 1)):
            got = self.at(self.chip(sign * d), 1 - h["core"], way if d == 4 else None)
            k = 1 + way * 4 + (d - 1)
            self.wait_at(got, self.ps.at[k], self.pr.at[k], h["partner"])

    def drain(self):
        for copy in self.sent:
            copy.wait_send()


def kernel(
    value_h, gate_h, taps_h, gain_h, shift_h, wc_h, x_h, mgain_h, routes_h, rw_h, wg_h, wu_h, wd_h, sg_h, su_h, sd_h,
    conv_o, moe_o,
    value, gate, taps, gain, shift, wc, x, mgain, routes, rw, wg, wu, wd, sg, su, sd,
    pad, halo_out, halo_in, filt, stat, normed, slot, wslot, onehot, packed, chi, clo,
    dbuf, hbuf, cbuf, gacc, uacc, oacc, outb, rbuf,
    load, misc, sr, sl, rr, rl, ps, pr,
):
    ep, tp = lax.axis_index("ep"), lax.axis_index("tp")
    z, xx = lax.div(ep, NX), lax.rem(ep, NX)
    y, core = lax.div(tp, NC), lax.rem(tp, NC)
    here = {
        "ep": ep, "y": y, "core": core,
        "right": lax.rem(y + 1, NY) * NC + core,
        "left": lax.rem(y + NY - 1, NY) * NC + core,
        "partner": y * NC + (1 - core),
    }

    def peer(rho, sign):
        q, dx = lax.div(rho, NX), lax.rem(rho, NX)
        odd = lax.rem(q, 2)
        dz = odd * lax.div(q + 1, 2) + (1 - odd) * lax.rem(NZ - lax.div(q, 2), NZ)
        return lax.rem(z + sign * dz + NZ, NZ) * NX + lax.rem(xx + sign * dx + NX, NX)

    loads = [
        pltpu.make_async_copy(a, b, load.at[i])
        for i, (a, b) in enumerate(
            (
                (x_h, x), (mgain_h, mgain), (routes_h, routes), (value_h, value), (gate_h, gate), (taps_h, taps),
                (gain_h, gain), (shift_h, shift), (sg_h, sg), (su_h, su), (wg_h, wg), (wu_h, wu), (wc_h, wc),
                (wd_h, wd), (rw_h, rw), (sd_h, sd),
            )
        )
    ]
    for copy in loads:
        copy.start()

    barrier = pltpu.get_barrier_semaphore()

    def greet_tp(r, carry):
        pl.semaphore_signal(barrier, inc=1, device_id=(ep, lax.rem(tp + r, N_TP)), device_id_type=MESH)
        return carry

    def greet_ep(r, carry):
        pl.semaphore_signal(barrier, inc=1, device_id=(lax.rem(ep + r, N_EP), tp), device_id_type=MESH)
        return carry

    lax.fori_loop(1, N_TP, greet_tp, 0)
    lax.fori_loop(1, N_EP, greet_ep, 0)

    for i in range(3):
        loads[i].wait()
    for r in range(0, TOK, 32):
        rows = x[r : r + 32, :].astype(F32)
        mean = jnp.mean(rows * rows, axis=1, keepdims=True)
        normed[r : r + 32, :] = (rows * lax.rsqrt(mean + 1e-06) * mgain[...]).astype(BF16)
    rho = lax.broadcasted_iota(jnp.int32, (N_EP, TOK), 0)
    q, dx = rho >> 2, rho & 3
    dz = jnp.where((q & 1) == 1, (q + 1) >> 1, (NZ - (q >> 1)) & 7)
    expert = ((z + dz) & 7) * NX + ((xx + dx) & 3)
    hits = jnp.zeros((N_EP, TOK), F32)
    for k in range(TOPK):
        hits = hits + jnp.where(routes[k : k + 1, :] == expert, 1.0, 0.0)
    before = jnp.where(
        lax.broadcasted_iota(jnp.int32, (TOK, TOK), 0) < lax.broadcasted_iota(jnp.int32, (TOK, TOK), 1), 1.0, 0.0
    ).astype(BF16)
    rank = dot(hits.astype(BF16), before)
    slot[...] = jnp.where(hits > 0.5, rank, -1.0)
    place = lax.broadcasted_iota(jnp.int32, (CAP, TOK), 0).astype(F32)
    for r in range(N_EP):
        onehot[r * CAP : (r + 1) * CAP, :] = jnp.where(slot[r : r + 1, :] == place, 1.0, 0.0).astype(BF16)
    mine = normed[:, pl.ds(pl.multiple_of(tp * CH, CH), CH)]
    packed[...] = dot(onehot[...], mine).astype(BF16)

    loads[3].wait()
    loads[4].wait()
    glu = (value[...].astype(F32) * sigmoid(gate[...].astype(F32))).astype(BF16)
    pad[HALO:, :] = glu.astype(F32)
    halo_out[...] = glu[ROWS_A - HALO :, :]

    pl.semaphore_wait(barrier, N_TP - 1 + N_EP - 1)

    def dispatch(r, carry):
        pltpu.make_async_remote_copy(
            src_ref=packed.at[pl.ds(r * CAP, CAP)], dst_ref=dbuf.at[tp, pl.ds(r * CAP, CAP)],
            send_sem=misc.at[0], recv_sem=misc.at[1], device_id=(peer(r, 1), tp), device_id_type=MESH,
        ).start()
        return carry

    halo = pltpu.make_async_remote_copy(
        src_ref=halo_out, dst_ref=halo_in, send_sem=misc.at[2], recv_sem=misc.at[3],
        device_id=(lax.rem(ep + 1, N_EP), tp), device_id_type=MESH,
    )
    halo.start()
    lax.fori_loop(1, N_EP, dispatch, 0)
    dbuf[tp, 0:CAP, :] = packed[0:CAP, :]

    loads[8].wait()
    loads[9].wait()
    shared = silu(dot(sg[...], normed[...], NT)) * dot(su[...], normed[...], NT)
    cbuf[tp, ROWS_A:, :] = shared.astype(BF16)

    loads[5].wait()
    loads[6].wait()
    loads[7].wait()
    halo.wait_recv()
    pad[:HALO, :] = halo_in[...].astype(F32) * jnp.where(ep > 0, 1.0, 0.0)
    for b in range(0, ROWS_A, 64):
        total = jnp.zeros((64, CH), F32)
        for j in range(TAPS):
            first = b + j + HALO - (TAPS - 1)
            total = total + taps[j : j + 1, :] * pad[first : first + 64, :]
        filt[b : b + 64, :] = total
    ones = jnp.ones((8, CH), F32)
    for r in range(4):
        part = filt[r * 128 : (r + 1) * 128, :]
        stat[0, r : r + 1, :] = dot(ones, part, NT, lax.Precision.HIGHEST)[0:1, :]
        stat[0, 4 + r : 5 + r, :] = dot(ones, part * part, NT, lax.Precision.HIGHEST)[0:1, :]

    def sums(r, carry):
        pltpu.make_async_remote_copy(
            src_ref=stat.at[0], dst_ref=stat.at[r], send_sem=misc.at[4], recv_sem=misc.at[5],
            device_id=(ep, lax.rem(tp + r, N_TP)), device_id_type=MESH,
        ).start()
        return carry

    lax.fori_loop(1, N_TP, sums, 0)

    sems = (sr, sl, rr, rl, ps, pr)
    ring_d = Ring(
        0, lambda t: dbuf.at[t], lambda t, i: dbuf.at[t, pl.ds(i * (SLOTS // 2), SLOTS // 2)], sems, here
    )
    ring_c = Ring(
        1, lambda t: cbuf.at[t], lambda t, i: cbuf.at[t, pl.ds(i * (CBROWS // 2), CBROWS // 2)], sems, here
    )
    ring_h = [
        Ring(
            2 + g,
            lambda t, g=g: hbuf.at[t, pl.ds(g * GROWS, GROWS)],
            lambda t, i, g=g: hbuf.at[t, pl.ds(g * GROWS + i * (GROWS // 2), GROWS // 2)],
            sems, here,
        )
        for g in range(GROUPS)
    ]

    arrived = pltpu.make_async_remote_copy(
        src_ref=packed.at[pl.ds(CAP, SLOTS - CAP)], dst_ref=dbuf.at[tp, pl.ds(CAP, SLOTS - CAP)],
        send_sem=misc.at[0], recv_sem=misc.at[1], device_id=(ep, here["right"]), device_id_type=MESH,
    )
    arrived.wait_recv()
    ring_d.own()

    summed = pltpu.make_async_remote_copy(
        src_ref=stat.at[pl.ds(1, N_TP - 1)], dst_ref=stat.at[pl.ds(1, N_TP - 1)],
        send_sem=misc.at[4], recv_sem=misc.at[5], device_id=(ep, here["right"]), device_id_type=MESH,
    )
    summed.wait_recv()
    total = stat[0]
    for r in range(1, N_TP):
        total = total + stat[r]
    total = total * (1.0 / D)
    mean, square = total[0:4, :], total[4:8, :]
    scale = lax.rsqrt(square - mean * mean + 1e-05)
    turned = jnp.concatenate([mean, scale], axis=0).T
    for r in range(4):
        part = filt[r * 128 : (r + 1) * 128, :]
        part = (part - turned[:, r : r + 1]) * turned[:, 4 + r : 5 + r]
        cbuf[tp, r * 128 : (r + 1) * 128, :] = silu(part * gain[...] + shift[...]).astype(BF16)
    ring_c.own()

    def gate_up(chip, g, first):
        rows = pl.ds(pl.multiple_of(g * GROWS, GROWS), GROWS)
        lhs = jnp.concatenate([dbuf[chip * NC, rows, :], dbuf[chip * NC + 1, rows, :]], axis=1)
        depth = pl.ds(pl.multiple_of(chip * NC * CH, NC * CH), NC * CH)
        a, b = dot(lhs, wg[depth, :]), dot(lhs, wu[depth, :])
        if first:
            gacc[rows, :] = a
            uacc[rows, :] = b
        else:
            gacc[rows, :] += a
            uacc[rows, :] += b

    def all_groups(chip, first=False):
        def step(g, carry):
            gate_up(chip, g, first)
            return carry

        lax.fori_loop(0, GROUPS, step, 0)

    loads[10].wait()
    loads[11].wait()
    ring_d.from_partner(0)
    all_groups(y, True)
    for d in range(1, 4):
        ring_d.stage(d)
        ring_c.stage(d)
        ring_d.from_partner(d)
        all_groups(ring_d.chip(-d))
        all_groups(ring_d.chip(d))

    def hidden(g):
        gate_up(ring_d.chip(4), g, False)
        rows = slice(g * GROWS, (g + 1) * GROWS)
        hbuf[tp, rows, :] = (silu(gacc[rows, :]) * uacc[rows, :]).astype(BF16)

    ring_d.stage(4)
    ring_d.from_partner(4)
    hidden(3)
    ring_h[3].own()
    hidden(2)
    ring_h[2].own()
    ring_c.stage(4)
    hidden(1)
    hidden(0)

    loads[14].wait()
    weight = jnp.zeros((N_EP, TOK), F32)
    for k in range(TOPK):
        weight = weight + jnp.where(routes[k : k + 1, :] == expert, rw[k : k + 1, :], 0.0)
    wslot[...] = weight
    for r in range(N_EP):
        w = wslot[r : r + 1, :]
        high = w.astype(BF16).astype(F32)
        hot = onehot[r * CAP : (r + 1) * CAP, :].astype(F32)
        chi[r * CAP : (r + 1) * CAP, :] = (hot * high).astype(BF16)
        clo[r * CAP : (r + 1) * CAP, :] = (hot * (w - high)).astype(BF16)

    loads[13].wait()

    def down(g, chip, first):
        rows = slice(g * GROWS, (g + 1) * GROWS)
        lhs = jnp.concatenate([hbuf[chip * NC, rows, :], hbuf[chip * NC + 1, rows, :]], axis=1)
        depth = pl.ds(pl.multiple_of(chip * NC * HID, NC * HID), NC * HID)
        a = dot(lhs, wd[depth, :])
        if first:
            oacc[rows, :] = a
        else:
            oacc[rows, :] += a

    def give_back(g):
        rows = slice(g * GROWS, (g + 1) * GROWS)
        outb[rows, :] = oacc[rows, :].astype(BF16)

        def back(r, carry):
            pltpu.make_async_remote_copy(
                src_ref=outb.at[pl.ds(r * CAP, CAP)], dst_ref=rbuf.at[pl.ds(r * CAP, CAP)],
                send_sem=misc.at[6], recv_sem=misc.at[7], device_id=(peer(r, -1), tp), device_id_type=MESH,
            ).start()
            return carry

        per = GROWS // CAP
        lax.fori_loop(max(1, g * per), (g + 1) * per, back, 0)

    def h_stage(g, d):
        ring_h[g].stage(d)
        ring_h[g].from_partner(d)
        if d < 4:
            down(g, ring_d.chip(-d), False)
        down(g, ring_d.chip(d), False)

    for pair in ((3, 2), (1, 0)):
        for g in pair:
            ring_h[g].from_partner(0)
            down(g, y, True)
        for d in range(1, 5):
            for i, g in enumerate(pair):
                h_stage(g, d)
                if d == 3 and pair == (3, 2):
                    ring_h[1 - i].own()
                if d == 4:
                    give_back(g)
        if pair == (3, 2):
            loads[12].wait()
            for d in range(5):
                ring_c.from_partner(d)
            for b in range(0, ROWS_A, 256):
                total = jnp.zeros((256, CH), F32)
                for t in range(0, N_TP, 2):
                    lhs = jnp.concatenate([cbuf[t, b : b + 256, :], cbuf[t + 1, b : b + 256, :]], axis=1)
                    total = total + dot(lhs, wc[t * CH : (t + 2) * CH, :])
                conv_o[b : b + 256, :] = total.astype(BF16)

    loads[15].wait()
    mid = jnp.concatenate([cbuf[t, ROWS_A:, :] for t in range(N_TP)], axis=0)
    shared_sum = dot(mid, sd[...], TN)
    rbuf[0:CAP, :] = outb[0:CAP, :]
    returned = pltpu.make_async_remote_copy(
        src_ref=outb.at[pl.ds(CAP, SLOTS - CAP)], dst_ref=rbuf.at[pl.ds(CAP, SLOTS - CAP)],
        send_sem=misc.at[6], recv_sem=misc.at[7], device_id=(ep, here["right"]), device_id_type=MESH,
    )
    returned.wait_recv()
    moe_o[...] = (dot(chi[...], rbuf[...], TN) + dot(clo[...], rbuf[...], TN) + shared_sum).astype(BF16)

    arrived.wait_send()
    halo.wait_send()
    summed.wait_send()
    returned.wait_send()
    for ring in (ring_d, ring_c, *ring_h):
        ring.drain()


def body(*args):
    (
        conv_value, conv_gate, conv_taps, norm_gain, norm_shift, conv_out_weight, moe_input, moe_gain, routes,
        route_weights, expert_gate, expert_up, expert_down, shared_gate, shared_up, shared_down,
    ) = args
    operands = (
        conv_value, conv_gate, conv_taps, norm_gain.reshape(1, CH), norm_shift.reshape(1, CH), conv_out_weight,
        moe_input, moe_gain.reshape(1, D), routes.T, route_weights.T, expert_gate[0], expert_up[0], expert_down[0],
        shared_gate.T, shared_up.T, shared_down,
    )
    vmem = pltpu.VMEM
    dma = pltpu.SemaphoreType.DMA
    rings = 2 + GROUPS
    return pl.pallas_call(
        kernel,
        out_shape=(jax.ShapeDtypeStruct((ROWS_A, CH), BF16), jax.ShapeDtypeStruct((TOK, CH), BF16)),
        in_specs=[pl.BlockSpec(memory_space=pl.ANY)] * len(operands),
        out_specs=(pl.BlockSpec(memory_space=pltpu.VMEM),) * 2,
        scratch_shapes=[vmem(o.shape, o.dtype) for o in operands]
        + [
            vmem((HALO + ROWS_A, CH), F32),
            vmem((HALO, CH), BF16),
            vmem((HALO, CH), BF16),
            vmem((ROWS_A, CH), F32),
            vmem((N_TP, 8, CH), F32),
            vmem((TOK, D), BF16),
            vmem((N_EP, TOK), F32),
            vmem((N_EP, TOK), F32),
            vmem((SLOTS, TOK), BF16),
            vmem((SLOTS, CH), BF16),
            vmem((SLOTS, TOK), BF16),
            vmem((SLOTS, TOK), BF16),
            vmem((N_TP, SLOTS, CH), BF16),
            vmem((N_TP, SLOTS, HID), BF16),
            vmem((N_TP, CBROWS, CH), BF16),
            vmem((SLOTS, HID), F32),
            vmem((SLOTS, HID), F32),
            vmem((SLOTS, CH), F32),
            vmem((SLOTS, CH), BF16),
            vmem((SLOTS, CH), BF16),
            dma((16,)),
            dma((8,)),
            dma((rings, 4)),
            dma((rings, 4)),
            dma((rings, 4)),
            dma((rings, 4)),
            dma((rings, 9)),
            dma((rings, 9)),
        ],
        compiler_params=pltpu.CompilerParams(
            collective_id=0, has_side_effects=True, vmem_limit_bytes=56 * 1024 * 1024
        ),
        cost_estimate=pl.CostEstimate(flops=5_000_000_000, bytes_accessed=8_000_000, transcendentals=0),
    )(*operands)


def solution(mesh):
    in_specs = (
        P("ep", "tp"),
        P("ep", "tp"),
        P(None, "tp"),
        P("tp"),
        P("tp"),
        P(None, "tp"),
        P("ep", None),
        P(),
        P("ep", None),
        P("ep", None),
        P("ep", None, "tp"),
        P("ep", None, "tp"),
        P("ep", None, "tp"),
        P(None, "tp"),
        P(None, "tp"),
        P(None, "tp"),
    )
    out_specs = (P("ep", "tp"), P("ep", "tp"))
    return jax.shard_map(body, mesh=mesh, in_specs=in_specs, out_specs=out_specs, check_vma=False)
```

```python
import functools

import jax
import jax.numpy as jnp
from jax import lax
from jax.experimental import pallas as pl
from jax.experimental.pallas import tpu as pltpu
from jax.sharding import PartitionSpec as P

MESH = pl.DeviceIdType.MESH
F32 = jnp.float32
BF16 = jnp.bfloat16

NZ, NX, NY, NC = 8, 4, 8, 2
N_EP, N_TP = NZ * NX, NY * NC
D = 2048
CH = D // N_TP
TAPS = 31
HALO = 32
ROWS_A = 512
TOK = 128
CAP = 32
SLOTS = N_EP * CAP
TOPK = 4
HID = 256
SH = 32
QROWS = NX * CAP
NEAR = 5
NEAR_BLOCKS = NEAR * NX
NEAR_ROWS = NEAR * QROWS
FAR_ROWS = SLOTS - NEAR_ROWS
WIDE = D // NC
GROUPS = ((0, 256), (512, 256), (768, 256), (384, 128), (256, 128))
CBROWS = ROWS_A + SH


def dot(a, b, dims=(((1,), (0,)), ((), ())), precision=None):
    return lax.dot_general(a, b, dims, precision=precision, preferred_element_type=F32)


NT = (((1,), (1,)), ((), ()))
TN = (((0,), (0,)), ((), ()))


def sigmoid(v):
    return 1.0 / (1.0 + jnp.exp(-v))


def silu(v):
    return v / (1.0 + jnp.exp(-v))


class Ring:
    def __init__(self, place, piece, half, sems, here):
        self.piece, self.half, self.here = piece, half, here
        self.sr, self.sl, self.rr, self.rl, self.ps, self.pr = (s.at[place] for s in sems)
        self.sent = []

    def chip(self, d):
        return lax.rem(self.here["y"] + d + 2 * NY, NY)

    def start(self, ref, send, recv, to):
        copy = pltpu.make_async_remote_copy(
            src_ref=ref, dst_ref=ref, send_sem=send, recv_sem=recv,
            device_id=(self.here["ep"], to), device_id_type=MESH,
        )
        copy.start()
        self.sent.append(copy)

    def wait_at(self, ref, send, recv, frm):
        pltpu.make_async_remote_copy(
            src_ref=ref, dst_ref=ref, send_sem=send, recv_sem=recv,
            device_id=(self.here["ep"], frm), device_id_type=MESH,
        ).wait_recv()

    def at(self, chip, core, part=None):
        t = chip * NC + core
        return self.piece(t) if part is None else self.half(t, part)

    def own(self):
        h = self.here
        mine = self.at(h["y"], h["core"])
        self.start(mine, self.sr.at[0], self.rr.at[0], h["right"])
        self.start(mine, self.sl.at[0], self.rl.at[0], h["left"])
        self.start(mine, self.ps.at[0], self.pr.at[0], h["partner"])

    def stage(self, d):
        h = self.here
        for way, (ss, rs, sign, to, frm) in enumerate(
            ((self.sr, self.rr, -1, h["right"], h["left"]), (self.sl, self.rl, 1, h["left"], h["right"]))
        ):
            chip = self.chip(sign * d)
            got = self.at(chip, h["core"], way if d == 4 else None)
            self.wait_at(got, ss.at[d - 1], rs.at[d - 1], frm)
            if d < 3:
                self.start(got, ss.at[d], rs.at[d], to)
            elif d == 3:
                self.start(self.at(chip, h["core"], way), ss.at[3], rs.at[3], to)
            k = 1 + way * 4 + (d - 1)
            self.start(got, self.ps.at[k], self.pr.at[k], h["partner"])

    def from_partner(self, d):
        h = self.here
        if d == 0:
            self.wait_at(self.at(h["y"], 1 - h["core"]), self.ps.at[0], self.pr.at[0], h["partner"])
            return
        for way, sign in enumerate((-1, 1)):
            got = self.at(self.chip(sign * d), 1 - h["core"], way if d == 4 else None)
            k = 1 + way * 4 + (d - 1)
            self.wait_at(got, self.ps.at[k], self.pr.at[k], h["partner"])

    def drain(self):
        for copy in self.sent:
            copy.wait_send()


def kernel(
    value_h, gate_h, taps_h, gain_h, shift_h, wc_h, x_h, mgain_h, routes_h, rw_h, wg_h, wu_h, wd_h, sg_h, su_h, sd_h,
    conv_h, moe_h,
    value, gate, taps, gain, shift, wc, x, mgain, routes, rw, wg, wu, wd, sg, su, sd, conv_o, moe_o,
    pad, halo_out, halo_in, filt, stat, normed, slot, wslot, onehot, wide, packed, chi, clo,
    nbuf, dbuf, hbuf, cbuf, oacc, outb, rbuf,
    load, misc, near_s, near_r, sr, sl, rr, rl, ps, pr,
):
    ep, tp = lax.axis_index("ep"), lax.axis_index("tp")
    z, xx = lax.div(ep, NX), lax.rem(ep, NX)
    y, core = lax.div(tp, NC), lax.rem(tp, NC)
    here = {
        "ep": ep, "y": y, "core": core,
        "right": lax.rem(y + 1, NY) * NC + core,
        "left": lax.rem(y + NY - 1, NY) * NC + core,
        "partner": y * NC + (1 - core),
    }

    def peer(rho, sign):
        q, dx = lax.div(rho, NX), lax.rem(rho, NX)
        odd = lax.rem(q, 2)
        dz = odd * lax.div(q + 1, 2) + (1 - odd) * lax.rem(NZ - lax.div(q, 2), NZ)
        return lax.rem(z + sign * dz + NZ, NZ) * NX + lax.rem(xx + sign * dx + NX, NX)

    def remote(src, dst, send, recv, to_ep, to_tp):
        return pltpu.make_async_remote_copy(
            src_ref=src, dst_ref=dst, send_sem=send, recv_sem=recv, device_id=(to_ep, to_tp), device_id_type=MESH
        )

    loads = [
        pltpu.make_async_copy(a, b, load.at[i])
        for i, (a, b) in enumerate(
            (
                (x_h, x), (mgain_h, mgain), (routes_h, routes), (value_h, value), (gate_h, gate), (taps_h, taps),
                (gain_h, gain), (shift_h, shift), (sg_h, sg), (su_h, su), (wg_h, wg), (wu_h, wu), (wc_h, wc),
                (wd_h, wd), (rw_h, rw), (sd_h, sd),
            )
        )
    ]
    for copy in loads:
        copy.start()

    barrier = pltpu.get_barrier_semaphore()

    def greet_tp(r, carry):
        pl.semaphore_signal(barrier, inc=1, device_id=(ep, lax.rem(tp + r, N_TP)), device_id_type=MESH)
        return carry

    def greet_ep(r, carry):
        pl.semaphore_signal(barrier, inc=1, device_id=(lax.rem(ep + r, N_EP), tp), device_id_type=MESH)
        return carry

    lax.fori_loop(1, N_TP, greet_tp, 0)
    lax.fori_loop(1, N_EP, greet_ep, 0)

    for i in range(3):
        loads[i].wait()
    for r in range(0, TOK, 32):
        rows = x[r : r + 32, :].astype(F32)
        mean = jnp.mean(rows * rows, axis=1, keepdims=True)
        normed[r : r + 32, :] = (rows * lax.rsqrt(mean + 1e-06) * mgain[...]).astype(BF16)
    rho = lax.broadcasted_iota(jnp.int32, (N_EP, TOK), 0)
    q, dx = rho >> 2, rho & 3
    dz = jnp.where((q & 1) == 1, (q + 1) >> 1, (NZ - (q >> 1)) & 7)
    expert = ((z + dz) & 7) * NX + ((xx + dx) & 3)
    hits = jnp.zeros((N_EP, TOK), F32)
    for k in range(TOPK):
        hits = hits + jnp.where(routes[k : k + 1, :] == expert, 1.0, 0.0)
    before = jnp.where(
        lax.broadcasted_iota(jnp.int32, (TOK, TOK), 0) < lax.broadcasted_iota(jnp.int32, (TOK, TOK), 1), 1.0, 0.0
    ).astype(BF16)
    rank = dot(hits.astype(BF16), before)
    slot[...] = jnp.where(hits > 0.5, rank, -1.0)
    place = lax.broadcasted_iota(jnp.int32, (CAP, TOK), 0).astype(F32)
    for r in range(N_EP):
        onehot[r * CAP : (r + 1) * CAP, :] = jnp.where(slot[r : r + 1, :] == place, 1.0, 0.0).astype(BF16)
    mine = normed[:, pl.ds(pl.multiple_of(tp * CH, CH), CH)]
    packed[...] = dot(onehot[NEAR_ROWS:, :], mine).astype(BF16)
    mine = normed[:, pl.ds(pl.multiple_of(core * WIDE, WIDE), WIDE)]

    def pack(i, carry):
        rows = pl.ds(pl.multiple_of(i * QROWS, QROWS), QROWS)
        wide[rows, :] = dot(onehot[rows, :], mine).astype(BF16)
        return carry

    lax.fori_loop(0, NEAR, pack, 0)
    nbuf[core, 0:CAP, :] = wide[0:CAP, :]

    loads[3].wait()
    loads[4].wait()
    glu = (value[...].astype(F32) * sigmoid(gate[...].astype(F32))).astype(BF16)
    pad[HALO:, :] = glu.astype(F32)
    halo_out[...] = glu[ROWS_A - HALO :, :]

    pl.semaphore_wait(barrier, N_TP - 1 + N_EP - 1)

    def dispatch(r, carry):
        rows = pl.ds((r - NEAR_BLOCKS) * CAP, CAP)
        remote(packed.at[rows], dbuf.at[tp, rows], misc.at[0], misc.at[1], peer(r, 1), tp).start()
        return carry

    def dispatch_near(q):
        def step(r, carry):
            rows = pl.ds(r * CAP, CAP)
            remote(wide.at[rows], nbuf.at[core, rows], near_s.at[q], near_r.at[q], peer(r, 1), tp).start()
            return carry

        lax.fori_loop(max(1, q * NX), (q + 1) * NX, step, 0)

    halo = remote(halo_out, halo_in, misc.at[2], misc.at[3], lax.rem(ep + 1, N_EP), tp)
    halo.start()
    lax.fori_loop(NEAR_BLOCKS, N_EP, dispatch, 0)
    for q in range(NEAR):
        dispatch_near(q)

    loads[8].wait()
    loads[9].wait()
    shared = silu(dot(sg[...], normed[...], NT)) * dot(su[...], normed[...], NT)
    cbuf[tp, ROWS_A:, :] = shared.astype(BF16)

    loads[5].wait()
    loads[6].wait()
    loads[7].wait()
    halo.wait_recv()
    pad[:HALO, :] = halo_in[...].astype(F32) * jnp.where(ep > 0, 1.0, 0.0)
    for b in range(0, ROWS_A, 64):
        total = jnp.zeros((64, CH), F32)
        for j in range(TAPS):
            first = b + j + HALO - (TAPS - 1)
            total = total + taps[j : j + 1, :] * pad[first : first + 64, :]
        filt[b : b + 64, :] = total
    ones = jnp.ones((8, CH), F32)
    for r in range(4):
        part = filt[r * 128 : (r + 1) * 128, :]
        stat[0, r : r + 1, :] = dot(ones, part, NT, lax.Precision.HIGHEST)[0:1, :]
        stat[0, 4 + r : 5 + r, :] = dot(ones, part * part, NT, lax.Precision.HIGHEST)[0:1, :]

    def sums(r, carry):
        remote(stat.at[0], stat.at[r], misc.at[4], misc.at[5], ep, lax.rem(tp + r, N_TP)).start()
        return carry

    lax.fori_loop(1, N_TP, sums, 0)

    sems = (sr, sl, rr, rl, ps, pr)
    ring_d = Ring(
        0, lambda t: dbuf.at[t], lambda t, i: dbuf.at[t, pl.ds(i * (FAR_ROWS // 2), FAR_ROWS // 2)], sems, here
    )
    ring_c = Ring(
        1, lambda t: cbuf.at[t], lambda t, i: cbuf.at[t, pl.ds(i * (CBROWS // 2), CBROWS // 2)], sems, here
    )
    ring_h = [
        Ring(
            2 + g,
            lambda t, a=a, n=n: hbuf.at[t, pl.ds(a, n)],
            lambda t, i, a=a, n=n: hbuf.at[t, pl.ds(a + i * (n // 2), n // 2)],
            sems, here,
        )
        for g, (a, n) in enumerate(GROUPS)
    ]

    arrived = remote(packed, dbuf.at[tp], misc.at[0], misc.at[1], ep, here["right"])
    arrived.wait_recv()
    ring_d.own()

    rest = pl.ds(1, N_TP - 1)
    summed = remote(stat.at[rest], stat.at[rest], misc.at[4], misc.at[5], ep, here["right"])
    summed.wait_recv()
    total = stat[0]
    for r in range(1, N_TP):
        total = total + stat[r]
    total = total * (1.0 / D)
    mean, square = total[0:4, :], total[4:8, :]
    scale = lax.rsqrt(square - mean * mean + 1e-05)
    turned = jnp.concatenate([mean, scale], axis=0).T
    for r in range(4):
        part = filt[r * 128 : (r + 1) * 128, :]
        part = (part - turned[:, r : r + 1]) * turned[:, 4 + r : 5 + r]
        cbuf[tp, r * 128 : (r + 1) * 128, :] = silu(part * gain[...] + shift[...]).astype(BF16)
    ring_c.own()

    passed = []
    landed = []

    def take_near(q):
        first = max(CAP, q * QROWS)
        rows = pl.ds(first, (q + 1) * QROWS - first)
        copy = remote(wide.at[rows], nbuf.at[core, rows], near_s.at[q], near_r.at[q], ep, here["right"])
        copy.wait_recv()
        landed.append(copy)
        rows = pl.ds(q * QROWS, QROWS)
        copy = remote(
            nbuf.at[core, rows], nbuf.at[core, rows], near_s.at[NEAR + q], near_r.at[NEAR + q], ep, here["partner"]
        )
        copy.start()
        passed.append(copy)

    def near_from_partner(q):
        rows = pl.ds(q * QROWS, QROWS)
        remote(
            nbuf.at[1 - core, rows], nbuf.at[1 - core, rows], near_s.at[NEAR + q], near_r.at[NEAR + q],
            ep, here["partner"],
        ).wait_recv()

    def hidden(q):
        if q < NEAR:
            near_from_partner(q)
            rows = slice(q * QROWS, (q + 1) * QROWS)
            a = dot(nbuf[0, rows, :], wg[:WIDE, :]) + dot(nbuf[1, rows, :], wg[WIDE:, :])
            b = dot(nbuf[0, rows, :], wu[:WIDE, :]) + dot(nbuf[1, rows, :], wu[WIDE:, :])
        else:
            rows = slice((q - NEAR) * QROWS, (q - NEAR + 1) * QROWS)
            lhs = jnp.concatenate([dbuf[t, rows, :] for t in range(N_TP)], axis=1)
            a, b = dot(lhs, wg[...]), dot(lhs, wu[...])
        hbuf[tp, q * QROWS : (q + 1) * QROWS, :] = (silu(a) * b).astype(BF16)

    def down(g, chip, first):
        a, n = GROUPS[g]
        rows = slice(a, a + n)
        lhs = jnp.concatenate([hbuf[chip * NC, rows, :], hbuf[chip * NC + 1, rows, :]], axis=1)
        depth = pl.ds(pl.multiple_of(chip * NC * HID, NC * HID), NC * HID)
        a = dot(lhs, wd[depth, :])
        if first:
            oacc[rows, :] = a
        else:
            oacc[rows, :] += a

    def give_back(g):
        a, n = GROUPS[g]
        outb[a : a + n, :] = oacc[a : a + n, :].astype(BF16)

        def back(r, carry):
            rows = pl.ds(r * CAP, CAP)
            remote(outb.at[rows], rbuf.at[rows], misc.at[6], misc.at[7], peer(r, -1), tp).start()
            return carry

        lax.fori_loop(max(1, a // CAP), (a + n) // CAP, back, 0)

    def h_own(g):
        ring_h[g].from_partner(0)
        down(g, y, True)

    def h_stage(g, d):
        ring_h[g].stage(d)
        ring_h[g].from_partner(d)
        if d < 4:
            down(g, ring_d.chip(-d), False)
        down(g, ring_d.chip(d), False)

    take_near(0)
    take_near(1)
    ring_d.stage(1)
    ring_c.stage(1)
    loads[10].wait()
    loads[11].wait()
    hidden(0)
    hidden(1)
    ring_h[0].own()
    ring_d.stage(2)
    ring_c.stage(2)
    loads[13].wait()
    h_own(0)
    h_stage(0, 1)
    take_near(2)
    take_near(3)
    ring_d.stage(3)
    ring_c.stage(3)
    h_stage(0, 2)
    take_near(4)
    ring_d.stage(4)
    h_stage(0, 3)
    for d in range(5):
        ring_d.from_partner(d)
    hidden(4)
    hidden(5)
    ring_h[1].own()
    hidden(6)
    hidden(7)
    ring_h[2].own()
    ring_c.stage(4)
    h_stage(0, 4)
    give_back(0)
    hidden(2)
    hidden(3)

    loads[14].wait()
    weight = jnp.zeros((N_EP, TOK), F32)
    for k in range(TOPK):
        weight = weight + jnp.where(routes[k : k + 1, :] == expert, rw[k : k + 1, :], 0.0)
    wslot[...] = weight
    for r in range(N_EP):
        w = wslot[r : r + 1, :]
        high = w.astype(BF16).astype(F32)
        hot = onehot[r * CAP : (r + 1) * CAP, :].astype(F32)
        chi[r * CAP : (r + 1) * CAP, :] = (hot * high).astype(BF16)
        clo[r * CAP : (r + 1) * CAP, :] = (hot * (w - high)).astype(BF16)

    for pair in ((1, 2), (3, 4)):
        for g in pair:
            h_own(g)
        for d in range(1, 5):
            for i, g in enumerate(pair):
                h_stage(g, d)
                if d == 3 and pair == (1, 2):
                    ring_h[3 + i].own()
                if d == 4:
                    give_back(g)
        if pair == (1, 2):
            loads[12].wait()
            for d in range(5):
                ring_c.from_partner(d)
            for b in range(0, ROWS_A, 256):
                total = jnp.zeros((256, CH), F32)
                for t in range(0, N_TP, 2):
                    lhs = jnp.concatenate([cbuf[t, b : b + 256, :], cbuf[t + 1, b : b + 256, :]], axis=1)
                    total = total + dot(lhs, wc[t * CH : (t + 2) * CH, :])
                conv_o[b : b + 256, :] = total.astype(BF16)
            conv_out = pltpu.make_async_copy(conv_o, conv_h, load.at[16])
            conv_out.start()
            loads[15].wait()
            mid = jnp.concatenate([cbuf[t, ROWS_A:, :] for t in range(N_TP)], axis=0)
            shared_sum = dot(mid, sd[...], TN)

    rbuf[0:CAP, :] = outb[0:CAP, :]
    rest = pl.ds(CAP, SLOTS - CAP)
    returned = remote(outb.at[rest], rbuf.at[rest], misc.at[6], misc.at[7], ep, here["right"])
    returned.wait_recv()
    moe_o[...] = (dot(chi[...], rbuf[...], TN) + dot(clo[...], rbuf[...], TN) + shared_sum).astype(BF16)
    moe_out = pltpu.make_async_copy(moe_o, moe_h, load.at[17])
    moe_out.start()

    for copy in (arrived, halo, summed, returned, *landed, *passed):
        copy.wait_send()
    for ring in (ring_d, ring_c, *ring_h):
        ring.drain()
    conv_out.wait()
    moe_out.wait()


def body(*args):
    (
        conv_value, conv_gate, conv_taps, norm_gain, norm_shift, conv_out_weight, moe_input, moe_gain, routes,
        route_weights, expert_gate, expert_up, expert_down, shared_gate, shared_up, shared_down,
    ) = args
    operands = (
        conv_value, conv_gate, conv_taps, norm_gain.reshape(1, CH), norm_shift.reshape(1, CH), conv_out_weight,
        moe_input, moe_gain.reshape(1, D), routes.T, route_weights.T, expert_gate[0], expert_up[0], expert_down[0],
        shared_gate.T, shared_up.T, shared_down,
    )
    vmem = pltpu.VMEM
    dma = pltpu.SemaphoreType.DMA
    rings = 2 + len(GROUPS)
    outs = (jax.ShapeDtypeStruct((ROWS_A, CH), BF16), jax.ShapeDtypeStruct((TOK, CH), BF16))
    return pl.pallas_call(
        kernel,
        out_shape=outs,
        in_specs=[pl.BlockSpec(memory_space=pl.ANY)] * len(operands),
        out_specs=(pl.BlockSpec(memory_space=pl.ANY),) * 2,
        scratch_shapes=[vmem(o.shape, o.dtype) for o in (*operands, *outs)]
        + [
            vmem((HALO + ROWS_A, CH), F32),
            vmem((HALO, CH), BF16),
            vmem((HALO, CH), BF16),
            vmem((ROWS_A, CH), F32),
            vmem((N_TP, 8, CH), F32),
            vmem((TOK, D), BF16),
            vmem((N_EP, TOK), F32),
            vmem((N_EP, TOK), F32),
            vmem((SLOTS, TOK), BF16),
            vmem((NEAR_ROWS, WIDE), BF16),
            vmem((FAR_ROWS, CH), BF16),
            vmem((SLOTS, TOK), BF16),
            vmem((SLOTS, TOK), BF16),
            vmem((NC, NEAR_ROWS, WIDE), BF16),
            vmem((N_TP, FAR_ROWS, CH), BF16),
            vmem((N_TP, SLOTS, HID), BF16),
            vmem((N_TP, CBROWS, CH), BF16),
            vmem((SLOTS, CH), F32),
            vmem((SLOTS, CH), BF16),
            vmem((SLOTS, CH), BF16),
            dma((18,)),
            dma((8,)),
            dma((2 * NEAR,)),
            dma((2 * NEAR,)),
            dma((rings, 4)),
            dma((rings, 4)),
            dma((rings, 4)),
            dma((rings, 4)),
            dma((rings, 9)),
            dma((rings, 9)),
        ],
        compiler_params=pltpu.CompilerParams(
            collective_id=0, has_side_effects=True, vmem_limit_bytes=56 * 1024 * 1024
        ),
        cost_estimate=pl.CostEstimate(flops=5_000_000_000, bytes_accessed=8_000_000, transcendentals=0),
    )(*operands)


def solution(mesh):
    in_specs = (
        P("ep", "tp"),
        P("ep", "tp"),
        P(None, "tp"),
        P("tp"),
        P("tp"),
        P(None, "tp"),
        P("ep", None),
        P(),
        P("ep", None),
        P("ep", None),
        P("ep", None, "tp"),
        P("ep", None, "tp"),
        P("ep", None, "tp"),
        P(None, "tp"),
        P(None, "tp"),
        P(None, "tp"),
    )
    out_specs = (P("ep", "tp"), P("ep", "tp"))
    return jax.shard_map(body, mesh=mesh, in_specs=in_specs, out_specs=out_specs, check_vma=False)
```

```python
import functools

import jax
import jax.numpy as jnp
from jax import lax
from jax.experimental import pallas as pl
from jax.experimental.pallas import tpu as pltpu
from jax.sharding import PartitionSpec as P

MESH = pl.DeviceIdType.MESH
F32 = jnp.float32
BF16 = jnp.bfloat16

NZ, NX, NY, NC = 8, 4, 8, 2
N_EP, N_TP = NZ * NX, NY * NC
D = 2048
CH = D // N_TP
TAPS = 31
HALO = 32
ROWS_A = 512
TOK = 128
CAP = 32
SLOTS = N_EP * CAP
TOPK = 4
HID = 256
SH = 32
QROWS = NX * CAP
NEAR = 5
NEAR_BLOCKS = NEAR * NX
NEAR_ROWS = NEAR * QROWS
FAR_ROWS = SLOTS - NEAR_ROWS
WIDE = D // NC
GROUPS = ((0, 128), (640, 384), (384, 256), (128, 256))
CBROWS = ROWS_A + SH
CSPLIT = ROWS_A // 2


def dot(a, b, dims=(((1,), (0,)), ((), ())), precision=None):
    return lax.dot_general(a, b, dims, precision=precision, preferred_element_type=F32)


NT = (((1,), (1,)), ((), ()))
TN = (((0,), (0,)), ((), ()))


def sigmoid(v):
    return 1.0 / (1.0 + jnp.exp(-v))


def silu(v):
    return v / (1.0 + jnp.exp(-v))


class Ring:
    def __init__(self, place, buffer, first, rows, sems, here):
        self.buffer, self.first, self.rows, self.here = buffer, first, rows, here
        send, rr, rl, pr = sems
        self.send = send.at[place]
        self.rr, self.rl, self.pr = rr.at[place], rl.at[place], pr.at[place]

    def chip(self, d):
        return lax.rem(self.here["y"] + d + 2 * NY, NY)

    def remote(self, ref, recv, to):
        return pltpu.make_async_remote_copy(
            src_ref=ref, dst_ref=ref, send_sem=self.send, recv_sem=recv,
            device_id=(self.here["ep"], to), device_id_type=MESH,
        )

    def at(self, chip, core, part=None):
        if part is None:
            return self.buffer.at[chip * NC + core, pl.ds(self.first, self.rows)]
        half = self.rows // 2
        return self.buffer.at[chip * NC + core, pl.ds(self.first + part * half, half)]

    def many(self, n):
        return self.buffer.at[pl.ds(0, n), pl.ds(self.first, self.rows)]

    def own(self):
        h = self.here
        mine = self.at(h["y"], h["core"])
        self.remote(mine, self.rr.at[0], h["right"]).start()
        self.remote(mine, self.rl.at[0], h["left"]).start()
        self.remote(mine, self.pr.at[0], h["partner"]).start()

    def stage(self, d):
        h = self.here
        for way, (rs, sign, to) in enumerate(((self.rr, -1, h["right"]), (self.rl, 1, h["left"]))):
            chip = self.chip(sign * d)
            got = self.at(chip, h["core"], way if d == 4 else None)
            self.remote(got, rs.at[d - 1], to).wait_recv()
            if d < 3:
                self.remote(got, rs.at[d], to).start()
            elif d == 3:
                self.remote(self.at(chip, h["core"], way), rs.at[3], to).start()
            self.remote(got, self.pr.at[d], h["partner"]).start()

    def from_partner(self, d):
        got = self.many(2 if 0 < d < 4 else 1)
        self.remote(got, self.pr.at[d], self.here["partner"]).wait_recv()

    def drain(self):
        self.remote(self.many(N_TP - 1), self.pr.at[0], self.here["partner"]).wait_send()


def kernel(
    value_h, gate_h, taps_h, gain_h, shift_h, wc_h, x_h, mgain_h, routes_h, rw_h, wg_h, wu_h, wd_h, sg_h, su_h, sd_h,
    conv_o, moe_o,
    value, gate, taps, gain, shift, wc, x, mgain, routes, rw, wg, wu, wd, sg, su, sd,
    pad, halo_out, halo_in, filt, stat, normed, slot, wslot, onehot, wide, packed, chi, clo,
    nbuf, dbuf, hbuf, cbuf, oacc, outb, rbuf,
    load, misc, near_s, near_r, back_s, back_r, send, rr, rl, pr,
):
    ep, tp = lax.axis_index("ep"), lax.axis_index("tp")
    z, xx = lax.div(ep, NX), lax.rem(ep, NX)
    y, core = lax.div(tp, NC), lax.rem(tp, NC)
    here = {
        "ep": ep, "y": y, "core": core,
        "right": lax.rem(y + 1, NY) * NC + core,
        "left": lax.rem(y + NY - 1, NY) * NC + core,
        "partner": y * NC + (1 - core),
    }

    def peer(rho, sign):
        q, dx = lax.div(rho, NX), lax.rem(rho, NX)
        odd = lax.rem(q, 2)
        dz = odd * lax.div(q + 1, 2) + (1 - odd) * lax.rem(NZ - lax.div(q, 2), NZ)
        return lax.rem(z + sign * dz + NZ, NZ) * NX + lax.rem(xx + sign * dx + NX, NX)

    def remote(src, dst, send, recv, to_ep, to_tp):
        return pltpu.make_async_remote_copy(
            src_ref=src, dst_ref=dst, send_sem=send, recv_sem=recv, device_id=(to_ep, to_tp), device_id_type=MESH
        )

    loads = [
        pltpu.make_async_copy(a, b, load.at[i])
        for i, (a, b) in enumerate(
            (
                (x_h, x), (mgain_h, mgain), (routes_h, routes), (value_h, value), (gate_h, gate), (taps_h, taps),
                (gain_h, gain), (shift_h, shift), (sg_h, sg), (su_h, su), (wg_h, wg), (wu_h, wu), (wc_h, wc),
                (wd_h, wd), (rw_h, rw), (sd_h, sd),
            )
        )
    ]
    for copy in loads[:5]:
        copy.start()

    barrier = pltpu.get_barrier_semaphore()

    def greet_tp(r, carry):
        pl.semaphore_signal(barrier, inc=1, device_id=(ep, lax.rem(tp + r, N_TP)), device_id_type=MESH)
        return carry

    def greet_ep(r, carry):
        pl.semaphore_signal(barrier, inc=1, device_id=(lax.rem(ep + r, N_EP), tp), device_id_type=MESH)
        return carry

    lax.fori_loop(1, N_EP, greet_ep, 0)
    lax.fori_loop(1, N_TP, greet_tp, 0)

    for copy in loads[5:]:
        copy.start()

    for i in range(3):
        loads[i].wait()
    for r in range(0, TOK, 32):
        rows = x[r : r + 32, :].astype(F32)
        mean = jnp.mean(rows * rows, axis=1, keepdims=True)
        normed[r : r + 32, :] = (rows * lax.rsqrt(mean + 1e-06) * mgain[...]).astype(BF16)
    rho = lax.broadcasted_iota(jnp.int32, (N_EP, TOK), 0)
    q, dx = rho >> 2, rho & 3
    dz = jnp.where((q & 1) == 1, (q + 1) >> 1, (NZ - (q >> 1)) & 7)
    expert = ((z + dz) & 7) * NX + ((xx + dx) & 3)
    hits = jnp.zeros((N_EP, TOK), F32)
    for k in range(TOPK):
        hits = hits + jnp.where(routes[k : k + 1, :] == expert, 1.0, 0.0)
    before = jnp.where(
        lax.broadcasted_iota(jnp.int32, (TOK, TOK), 0) < lax.broadcasted_iota(jnp.int32, (TOK, TOK), 1), 1.0, 0.0
    ).astype(BF16)
    rank = dot(hits.astype(BF16), before)
    slot[...] = jnp.where(hits > 0.5, rank, -1.0)
    place = lax.broadcasted_iota(jnp.int32, (CAP, TOK), 0).astype(F32)
    for r in range(N_EP):
        onehot[r * CAP : (r + 1) * CAP, :] = jnp.where(slot[r : r + 1, :] == place, 1.0, 0.0).astype(BF16)

    def pack(q):
        rows = slice(q * QROWS, (q + 1) * QROWS)
        mine = normed[:, pl.ds(pl.multiple_of(core * WIDE, WIDE), WIDE)]
        wide[rows, :] = dot(onehot[rows, :], mine).astype(BF16)

    pack(0)

    loads[3].wait()
    loads[4].wait()
    glu = (value[...].astype(F32) * sigmoid(gate[...].astype(F32))).astype(BF16)
    pad[HALO:, :] = glu.astype(F32)
    halo_out[...] = glu[ROWS_A - HALO :, :]
    halo = remote(halo_out, halo_in, misc.at[2], misc.at[3], lax.rem(ep + 1, N_EP), tp)
    pl.semaphore_wait(barrier, N_TP - 1 + N_EP - 1)

    def dispatch(r, carry):
        rows = pl.ds((r - NEAR_BLOCKS) * CAP, CAP)
        remote(packed.at[rows], dbuf.at[tp, rows], misc.at[0], misc.at[1], peer(r, 1), tp).start()
        return carry

    def dispatch_near(q):
        def step(r, carry):
            rows = pl.ds(r * CAP, CAP)
            remote(wide.at[rows], nbuf.at[core, rows], near_s.at[q], near_r.at[q], peer(r, 1), tp).start()
            return carry

        lax.fori_loop(max(1, q * NX), (q + 1) * NX, step, 0)

    @pl.when(ep < N_EP - 1)
    def _():
        halo.start()

    dispatch_near(0)
    nbuf[core, 0:CAP, :] = wide[0:CAP, :]
    packed[...] = dot(onehot[NEAR_ROWS:, :], normed[:, pl.ds(pl.multiple_of(tp * CH, CH), CH)]).astype(BF16)
    lax.fori_loop(NEAR_BLOCKS, N_EP, dispatch, 0)
    for q in (1, 2):
        pack(q)
        dispatch_near(q)

    loads[8].wait()
    loads[9].wait()
    shared = silu(dot(sg[...], normed[...], NT)) * dot(su[...], normed[...], NT)
    cbuf[tp, ROWS_A:, :] = shared.astype(BF16)

    loads[5].wait()
    loads[6].wait()
    loads[7].wait()
    pad[:HALO, :] = jnp.zeros((HALO, CH), F32)

    @pl.when(ep > 0)
    def _():
        halo.wait_recv()
        pad[:HALO, :] = halo_in[...].astype(F32)

    for b in range(0, ROWS_A, 64):
        total = jnp.zeros((64, CH), F32)
        for j in range(TAPS):
            first = b + j + HALO - (TAPS - 1)
            total = total + taps[j : j + 1, :] * pad[first : first + 64, :]
        filt[b : b + 64, :] = total
    ones = jnp.ones((8, CH), F32)
    for r in range(4):
        part = filt[r * 128 : (r + 1) * 128, :]
        stat[0, r : r + 1, :] = dot(ones, part, NT, lax.Precision.HIGHEST)[0:1, :]
        stat[0, 4 + r : 5 + r, :] = dot(ones, part * part, NT, lax.Precision.HIGHEST)[0:1, :]

    def sums(r, carry):
        remote(stat.at[0], stat.at[r], misc.at[4], misc.at[5], ep, lax.rem(tp + r, N_TP)).start()
        return carry

    lax.fori_loop(1, N_TP, sums, 0)

    sems = (send, rr, rl, pr)
    ring_d = Ring(0, dbuf, 0, FAR_ROWS, sems, here)
    ring_c = [Ring(1, cbuf, 0, CSPLIT, sems, here), Ring(2, cbuf, CSPLIT, CBROWS - CSPLIT, sems, here)]
    ring_h = [Ring(3 + g, hbuf, a, n, sems, here) for g, (a, n) in enumerate(GROUPS)]

    passed = []
    landed = []

    def take_near(q):
        first = max(CAP, q * QROWS)
        rows = pl.ds(first, (q + 1) * QROWS - first)
        copy = remote(wide.at[rows], nbuf.at[core, rows], near_s.at[q], near_r.at[q], ep, here["right"])
        copy.wait_recv()
        landed.append(copy)
        rows = pl.ds(q * QROWS, QROWS)
        copy = remote(
            nbuf.at[core, rows], nbuf.at[core, rows], near_s.at[NEAR + q], near_r.at[NEAR + q], ep, here["partner"]
        )
        copy.start()
        passed.append(copy)

    def near_from_partner(q):
        rows = pl.ds(q * QROWS, QROWS)
        remote(
            nbuf.at[1 - core, rows], nbuf.at[1 - core, rows], near_s.at[NEAR + q], near_r.at[NEAR + q],
            ep, here["partner"],
        ).wait_recv()

    def hidden(q):
        if q < NEAR:
            near_from_partner(q)
            rows = slice(q * QROWS, (q + 1) * QROWS)
            a = dot(nbuf[0, rows, :], wg[:WIDE, :]) + dot(nbuf[1, rows, :], wg[WIDE:, :])
            b = dot(nbuf[0, rows, :], wu[:WIDE, :]) + dot(nbuf[1, rows, :], wu[WIDE:, :])
        else:
            rows = slice((q - NEAR) * QROWS, (q - NEAR + 1) * QROWS)
            lhs = jnp.concatenate([dbuf[t, rows, :] for t in range(N_TP)], axis=1)
            a, b = dot(lhs, wg[...]), dot(lhs, wu[...])
        hbuf[tp, q * QROWS : (q + 1) * QROWS, :] = (silu(a) * b).astype(BF16)

    def down(g, chip, first):
        a, n = GROUPS[g]
        rows = slice(a, a + n)
        lhs = jnp.concatenate([hbuf[chip * NC, rows, :], hbuf[chip * NC + 1, rows, :]], axis=1)
        depth = pl.ds(pl.multiple_of(chip * NC * HID, NC * HID), NC * HID)
        a = dot(lhs, wd[depth, :])
        if first:
            oacc[rows, :] = a
        else:
            oacc[rows, :] += a

    def returned(g):
        first, end = max(CAP, GROUPS[g][0]), sum(GROUPS[g])
        rows = pl.ds(first, end - first)
        return remote(outb.at[rows], rbuf.at[rows], back_s.at[g], back_r.at[g], ep, here["right"])

    def combine(g):
        returned(g).wait_recv()
        a, n = GROUPS[g]
        rows = slice(a, a + n)
        return dot(chi[rows, :], rbuf[rows, :], TN) + dot(clo[rows, :], rbuf[rows, :], TN)

    def give_back(g):
        a, n = GROUPS[g]
        outb[a : a + n, :] = oacc[a : a + n, :].astype(BF16)

        def back(r, carry):
            rows = pl.ds(r * CAP, CAP)
            remote(outb.at[rows], rbuf.at[rows], back_s.at[g], back_r.at[g], peer(r, -1), tp).start()
            return carry

        lax.fori_loop(max(1, a // CAP), (a + n) // CAP, back, 0)

    def h_down(g, d):
        ring_h[g].from_partner(d)
        if d < 4:
            down(g, ring_d.chip(-d), d == 0)
        if d > 0:
            down(g, ring_d.chip(d), False)

    def conv_down(part, d):
        ring_c[part].from_partner(d)
        rows = slice(part * CSPLIT, (part + 1) * CSPLIT)
        for sign in (-1, 1)[0 if 0 < d < 4 else 1 :]:
            chip = ring_d.chip(sign * d)
            depth = pl.ds(pl.multiple_of(chip * NC * CH, NC * CH), NC * CH)
            lhs = jnp.concatenate([cbuf[chip * NC, rows, :], cbuf[chip * NC + 1, rows, :]], axis=1)
            product = dot(lhs, wc[depth, :])
            if d == 0:
                filt[rows, :] = product
            else:
                filt[rows, :] += product

    take_near(0)
    loads[10].wait()
    loads[11].wait()
    hidden(0)
    ring_h[0].own()
    arrived = remote(packed, dbuf.at[tp], misc.at[0], misc.at[1], ep, here["right"])
    arrived.wait_recv()
    ring_d.own()
    rest = pl.ds(1, N_TP - 1)
    summed = remote(stat.at[rest], stat.at[rest], misc.at[4], misc.at[5], ep, here["right"])
    summed.wait_recv()
    total = stat[0]
    for r in range(1, N_TP):
        total = total + stat[r]
    total = total * (1.0 / D)
    mean, square = total[0:4, :], total[4:8, :]
    scale = lax.rsqrt(square - mean * mean + 1e-05)
    turned = jnp.concatenate([mean, scale], axis=0).T
    for r in range(4):
        part = filt[r * 128 : (r + 1) * 128, :]
        part = (part - turned[:, r : r + 1]) * turned[:, 4 + r : 5 + r]
        cbuf[tp, r * 128 : (r + 1) * 128, :] = silu(part * gain[...] + shift[...]).astype(BF16)
    ring_c[0].own()
    ring_h[0].stage(1)
    ring_d.stage(1)
    ring_c[0].stage(1)
    loads[13].wait()
    h_down(0, 0)
    take_near(1)
    take_near(2)
    pack(3)
    dispatch_near(3)
    pack(4)
    dispatch_near(4)
    hidden(1)
    hidden(2)
    ring_h[3].own()
    ring_h[0].stage(2)
    ring_d.stage(2)
    ring_c[0].stage(2)
    h_down(0, 1)
    ring_h[0].stage(3)
    ring_d.stage(3)
    ring_c[0].stage(3)
    ring_h[3].stage(1)
    h_down(0, 2)
    h_down(3, 0)
    ring_d.stage(4)
    ring_h[0].stage(4)
    ring_c[0].stage(4)
    ring_h[3].stage(2)
    for d in range(5):
        ring_d.from_partner(d)
    hidden(5)
    hidden(6)
    hidden(7)
    ring_h[1].own()
    h_down(0, 3)
    h_down(0, 4)
    give_back(0)
    take_near(3)
    take_near(4)
    hidden(3)
    hidden(4)
    ring_h[2].own()
    ring_h[3].stage(3)
    h_down(3, 1)
    h_down(3, 2)
    ring_h[1].stage(1)
    ring_h[3].stage(4)
    ring_h[2].stage(1)
    h_down(3, 3)
    h_down(3, 4)
    give_back(3)
    h_down(1, 0)
    h_down(2, 0)
    ring_h[1].stage(2)
    ring_h[2].stage(2)
    ring_c[1].own()
    h_down(1, 1)
    h_down(2, 1)
    loads[12].wait()
    for d in range(5):
        conv_down(0, d)
    ring_h[1].stage(3)
    ring_h[2].stage(3)
    ring_c[1].stage(1)
    h_down(1, 2)
    h_down(2, 2)

    loads[14].wait()
    weight = jnp.zeros((N_EP, TOK), F32)
    for k in range(TOPK):
        weight = weight + jnp.where(routes[k : k + 1, :] == expert, rw[k : k + 1, :], 0.0)
    wslot[...] = weight
    for r in range(N_EP):
        w = wslot[r : r + 1, :]
        high = w.astype(BF16).astype(F32)
        hot = onehot[r * CAP : (r + 1) * CAP, :].astype(F32)
        chi[r * CAP : (r + 1) * CAP, :] = (hot * high).astype(BF16)
        clo[r * CAP : (r + 1) * CAP, :] = (hot * (w - high)).astype(BF16)
    ring_h[1].stage(4)
    ring_h[2].stage(4)
    ring_c[1].stage(2)
    h_down(1, 3)
    h_down(1, 4)
    give_back(1)
    h_down(2, 3)
    h_down(2, 4)
    give_back(2)
    ring_c[1].stage(3)
    for d in range(3):
        conv_down(1, d)
    loads[15].wait()

    rbuf[0:CAP, :] = outb[0:CAP, :]
    summed_up = combine(0) + combine(3)
    ring_c[1].stage(4)
    conv_down(1, 3)
    conv_down(1, 4)
    conv_o[...] = filt[...].astype(BF16)
    mid = jnp.concatenate([cbuf[t, ROWS_A:, :] for t in range(N_TP)], axis=0)
    summed_up = summed_up + dot(mid, sd[...], TN)
    moe_o[...] = (summed_up + combine(1) + combine(2)).astype(BF16)

    @pl.when(ep < N_EP - 1)
    def _():
        halo.wait_send()

    for copy in (arrived, summed, *[returned(g) for g in range(len(GROUPS))], *landed, *passed):
        copy.wait_send()
    for ring in (ring_d, *ring_c, *ring_h):
        ring.drain()


def body(*args):
    (
        conv_value, conv_gate, conv_taps, norm_gain, norm_shift, conv_out_weight, moe_input, moe_gain, routes,
        route_weights, expert_gate, expert_up, expert_down, shared_gate, shared_up, shared_down,
    ) = args
    operands = (
        conv_value, conv_gate, conv_taps, norm_gain.reshape(1, CH), norm_shift.reshape(1, CH), conv_out_weight,
        moe_input, moe_gain.reshape(1, D), routes.T, route_weights.T, expert_gate[0], expert_up[0], expert_down[0],
        shared_gate.T, shared_up.T, shared_down,
    )
    vmem = pltpu.VMEM
    dma = pltpu.SemaphoreType.DMA
    rings = 3 + len(GROUPS)
    outs = (vmem((ROWS_A, CH), BF16), vmem((TOK, CH), BF16))
    return pl.pallas_call(
        kernel,
        out_shape=outs,
        in_specs=[pl.BlockSpec(memory_space=pltpu.HBM)] * len(operands),
        out_specs=(pl.BlockSpec(memory_space=pltpu.VMEM),) * 2,
        scratch_shapes=[vmem(o.shape, o.dtype) for o in operands]
        + [
            vmem((HALO + ROWS_A, CH), F32),
            vmem((HALO, CH), BF16),
            vmem((HALO, CH), BF16),
            vmem((ROWS_A, CH), F32),
            vmem((N_TP, 8, CH), F32),
            vmem((TOK, D), BF16),
            vmem((N_EP, TOK), F32),
            vmem((N_EP, TOK), F32),
            vmem((SLOTS, TOK), BF16),
            vmem((NEAR_ROWS, WIDE), BF16),
            vmem((FAR_ROWS, CH), BF16),
            vmem((SLOTS, TOK), BF16),
            vmem((SLOTS, TOK), BF16),
            vmem((NC, NEAR_ROWS, WIDE), BF16),
            vmem((N_TP, FAR_ROWS, CH), BF16),
            vmem((N_TP, SLOTS, HID), BF16),
            vmem((N_TP, CBROWS, CH), BF16),
            vmem((SLOTS, CH), F32),
            vmem((SLOTS, CH), BF16),
            vmem((SLOTS, CH), BF16),
            dma((16,)),
            dma((6,)),
            dma((2 * NEAR,)),
            dma((2 * NEAR,)),
            dma((len(GROUPS),)),
            dma((len(GROUPS),)),
            dma((rings,)),
            dma((rings, 4)),
            dma((rings, 4)),
            dma((rings, 5)),
        ],
        compiler_params=pltpu.CompilerParams(
            collective_id=0, has_side_effects=True, vmem_limit_bytes=55 * 1024 * 1024
        ),
        cost_estimate=pl.CostEstimate(flops=5_000_000_000, bytes_accessed=8_000_000, transcendentals=0),
    )(*operands)


def solution(mesh):
    in_specs = (
        P("ep", "tp"),
        P("ep", "tp"),
        P(None, "tp"),
        P("tp"),
        P("tp"),
        P(None, "tp"),
        P("ep", None),
        P(),
        P("ep", None),
        P("ep", None),
        P("ep", None, "tp"),
        P("ep", None, "tp"),
        P("ep", None, "tp"),
        P(None, "tp"),
        P(None, "tp"),
        P(None, "tp"),
    )
    out_specs = (P("ep", "tp"), P("ep", "tp"))
    return jax.shard_map(body, mesh=mesh, in_specs=in_specs, out_specs=out_specs, check_vma=False)
```

```python
import functools

import jax
import jax.numpy as jnp
from jax import lax
from jax.experimental import pallas as pl
from jax.experimental.pallas import tpu as pltpu
from jax.sharding import PartitionSpec as P

MESH = pl.DeviceIdType.MESH
F32 = jnp.float32
BF16 = jnp.bfloat16

NZ, NX, NY, NC = 8, 4, 8, 2
N_EP, N_TP = NZ * NX, NY * NC
D = 2048
CH = D // N_TP
TAPS = 31
HALO = 32
ROWS_A = 512
TOK = 128
CAP = 32
SLOTS = N_EP * CAP
TOPK = 4
HID = 256
SH = 32
QROWS = NX * CAP
NEAR = 5
NEAR_BLOCKS = NEAR * NX
NEAR_ROWS = NEAR * QROWS
FAR_ROWS = SLOTS - NEAR_ROWS
WIDE = D // NC
GROUPS = ((0, 128), (640, 384), (384, 256), (128, 256))
CBROWS = ROWS_A + SH
CSPLIT = ROWS_A // 2


def dot(a, b, dims=(((1,), (0,)), ((), ())), precision=None):
    return lax.dot_general(a, b, dims, precision=precision, preferred_element_type=F32)


NT = (((1,), (1,)), ((), ()))
TN = (((0,), (0,)), ((), ()))


def sigmoid(v):
    return 1.0 / (1.0 + jnp.exp(-v))


def silu(v):
    return v / (1.0 + jnp.exp(-v))


class Ring:
    def __init__(self, place, buffer, first, rows, sems, here):
        self.buffer, self.first, self.rows, self.here = buffer, first, rows, here
        send, recv, pr = sems
        self.send, self.recv, self.pr = send.at[place], recv.at[place], pr.at[place]

    def chip(self, d):
        return lax.rem(self.here["y"] + d + 2 * NY, NY)

    def behind(self, d):
        return lax.rem(self.here["y"] - self.here["way"] * d + 2 * NY, NY)

    def remote(self, ref, recv, to):
        return pltpu.make_async_remote_copy(
            src_ref=ref, dst_ref=ref, send_sem=self.send, recv_sem=recv,
            device_id=(self.here["ep"], to), device_id_type=MESH,
        )

    def at(self, chip, core, halved=False):
        if not halved:
            return self.buffer.at[chip * NC + core, pl.ds(self.first, self.rows)]
        half = self.rows // 2
        first = pl.multiple_of(self.first + self.here["core"] * half, 16)
        return self.buffer.at[chip * NC + core, pl.ds(first, half)]

    def many(self, n):
        return self.buffer.at[pl.ds(0, n), pl.ds(self.first, self.rows)]

    def own(self):
        h = self.here
        mine = self.at(h["y"], h["core"])
        self.remote(mine, self.pr.at[0], h["partner"]).start()
        self.remote(mine, self.recv.at[0], h["next"]).start()

    def own2(self):
        h = self.here
        other = self.at(h["y"], 1 - h["core"])
        self.remote(other, self.pr.at[0], h["partner"]).wait_recv()
        self.remote(other, self.recv.at[1], h["next"]).start()

    def stage(self, d):
        h = self.here
        chip = self.behind(d)
        for j, core in enumerate((h["core"], 1 - h["core"])):
            got = self.at(chip, core, d == 4)
            self.remote(got, self.recv.at[2 * d - 2 + j], h["next"]).wait_recv()
            if d < 4:
                self.remote(self.at(chip, core, d == 3), self.recv.at[2 * d + j], h["next"]).start()
            self.remote(got, self.pr.at[d], h["partner"]).start()

    def from_partner(self, d):
        got = self.many(2 if d < 4 else 1)
        self.remote(got, self.pr.at[d], self.here["partner"]).wait_recv()

    def drain(self):
        self.remote(self.many(N_TP - 1), self.pr.at[0], self.here["partner"]).wait_send()


def kernel(
    value_h, gate_h, taps_h, gain_h, shift_h, wc_h, x_h, mgain_h, routes_h, rw_h, wg_h, wu_h, wd_h, sg_h, su_h, sd_h,
    conv_o, moe_o,
    value, gate, taps, gain, shift, wc, x, mgain, routes, rw, wg, wu, wd, sg, su, sd,
    pad, halo_out, halo_in, filt, stat, normed, slot, wslot, onehot, wide, packed, chi, clo,
    nbuf, dbuf, hbuf, cbuf, oacc, outb, rbuf,
    load, misc, near_s, near_r, back_s, back_r, send, recv, pr,
):
    ep, tp = lax.axis_index("ep"), lax.axis_index("tp")
    z, xx = lax.div(ep, NX), lax.rem(ep, NX)
    y, core = lax.div(tp, NC), lax.rem(tp, NC)
    here = {
        "ep": ep, "y": y, "core": core,
        "way": 1 - 2 * core,
        "next": lax.rem(y + 1 - 2 * core + NY, NY) * NC + core,
        "partner": y * NC + (1 - core),
    }

    def peer(rho, sign):
        q, dx = lax.div(rho, NX), lax.rem(rho, NX)
        odd = lax.rem(q, 2)
        dz = odd * lax.div(q + 1, 2) + (1 - odd) * lax.rem(NZ - lax.div(q, 2), NZ)
        return lax.rem(z + sign * dz + NZ, NZ) * NX + lax.rem(xx + sign * dx + NX, NX)

    def remote(src, dst, send, recv, to_ep, to_tp):
        return pltpu.make_async_remote_copy(
            src_ref=src, dst_ref=dst, send_sem=send, recv_sem=recv, device_id=(to_ep, to_tp), device_id_type=MESH
        )

    loads = [
        pltpu.make_async_copy(a, b, load.at[i])
        for i, (a, b) in enumerate(
            (
                (x_h, x), (mgain_h, mgain), (routes_h, routes), (value_h, value), (gate_h, gate), (taps_h, taps),
                (gain_h, gain), (shift_h, shift), (sg_h, sg), (su_h, su), (wg_h, wg), (wu_h, wu), (wc_h, wc),
                (wd_h, wd), (rw_h, rw), (sd_h, sd),
            )
        )
    ]
    for copy in loads[:5]:
        copy.start()

    barrier = pltpu.get_barrier_semaphore()

    def greet_tp(r, carry):
        pl.semaphore_signal(barrier, inc=1, device_id=(ep, lax.rem(tp + r, N_TP)), device_id_type=MESH)
        return carry

    def greet_ep(r, carry):
        pl.semaphore_signal(barrier, inc=1, device_id=(peer(N_EP - r, 1), tp), device_id_type=MESH)
        return carry

    lax.fori_loop(1, N_EP, greet_ep, 0)
    lax.fori_loop(1, N_TP, greet_tp, 0)

    for copy in loads[5:]:
        copy.start()

    for i in range(3):
        loads[i].wait()
    for r in range(0, TOK, 32):
        rows = x[r : r + 32, :].astype(F32)
        mean = jnp.mean(rows * rows, axis=1, keepdims=True)
        normed[r : r + 32, :] = (rows * lax.rsqrt(mean + 1e-06) * mgain[...]).astype(BF16)
    rho = lax.broadcasted_iota(jnp.int32, (N_EP, TOK), 0)
    q, dx = rho >> 2, rho & 3
    dz = jnp.where((q & 1) == 1, (q + 1) >> 1, (NZ - (q >> 1)) & 7)
    expert = ((z + dz) & 7) * NX + ((xx + dx) & 3)
    hits = jnp.zeros((N_EP, TOK), F32)
    for k in range(TOPK):
        hits = hits + jnp.where(routes[k : k + 1, :] == expert, 1.0, 0.0)
    before = jnp.where(
        lax.broadcasted_iota(jnp.int32, (TOK, TOK), 0) < lax.broadcasted_iota(jnp.int32, (TOK, TOK), 1), 1.0, 0.0
    ).astype(BF16)
    rank = dot(hits.astype(BF16), before)
    slot[...] = jnp.where(hits > 0.5, rank, -1.0)
    place = lax.broadcasted_iota(jnp.int32, (CAP, TOK), 0).astype(F32)
    for r in range(N_EP):
        onehot[r * CAP : (r + 1) * CAP, :] = jnp.where(slot[r : r + 1, :] == place, 1.0, 0.0).astype(BF16)

    def pack(q):
        rows = slice(q * QROWS, (q + 1) * QROWS)
        mine = normed[:, pl.ds(pl.multiple_of(core * WIDE, WIDE), WIDE)]
        wide[rows, :] = dot(onehot[rows, :], mine).astype(BF16)

    pack(0)
    packed[...] = dot(onehot[NEAR_ROWS:, :], normed[:, pl.ds(pl.multiple_of(tp * CH, CH), CH)]).astype(BF16)

    loads[3].wait()
    loads[4].wait()
    glu = (value[...].astype(F32) * sigmoid(gate[...].astype(F32))).astype(BF16)
    pad[HALO:, :] = glu.astype(F32)
    halo_out[...] = glu[ROWS_A - HALO :, :]
    halo = remote(halo_out, halo_in, misc.at[2], misc.at[3], lax.rem(ep + 1, N_EP), tp)
    pl.semaphore_wait(barrier, N_TP - 1 + N_EP - 1)

    def dispatch(r, carry):
        rows = pl.ds((r - NEAR_BLOCKS) * CAP, CAP)
        remote(packed.at[rows], dbuf.at[tp, rows], misc.at[0], misc.at[1], peer(r, 1), tp).start()
        return carry

    def dispatch_near(q):
        def step(r, carry):
            rows = pl.ds(r * CAP, CAP)
            remote(wide.at[rows], nbuf.at[core, rows], near_s.at[q], near_r.at[q], peer(r, 1), tp).start()
            return carry

        lax.fori_loop(max(1, q * NX), (q + 1) * NX, step, 0)

    @pl.when(ep < N_EP - 1)
    def _():
        halo.start()

    lax.fori_loop(NEAR_BLOCKS, N_EP, dispatch, 0)
    dispatch_near(0)
    nbuf[core, 0:CAP, :] = wide[0:CAP, :]
    for q in (1, 2):
        pack(q)

    loads[8].wait()
    loads[9].wait()
    shared = silu(dot(sg[...], normed[...], NT)) * dot(su[...], normed[...], NT)
    cbuf[tp, ROWS_A:, :] = shared.astype(BF16)

    loads[5].wait()
    loads[6].wait()
    loads[7].wait()
    pad[:HALO, :] = jnp.zeros((HALO, CH), F32)

    @pl.when(ep > 0)
    def _():
        halo.wait_recv()
        pad[:HALO, :] = halo_in[...].astype(F32)

    for b in range(0, ROWS_A, 64):
        total = jnp.zeros((64, CH), F32)
        for j in range(TAPS):
            first = b + j + HALO - (TAPS - 1)
            total = total + taps[j : j + 1, :] * pad[first : first + 64, :]
        filt[b : b + 64, :] = total
    ones = jnp.ones((8, CH), F32)
    for r in range(4):
        part = filt[r * 128 : (r + 1) * 128, :]
        stat[0, r : r + 1, :] = dot(ones, part, NT, lax.Precision.HIGHEST)[0:1, :]
        stat[0, 4 + r : 5 + r, :] = dot(ones, part * part, NT, lax.Precision.HIGHEST)[0:1, :]

    def sums(r, carry):
        remote(stat.at[0], stat.at[r], misc.at[4], misc.at[5], ep, lax.rem(tp + r, N_TP)).start()
        return carry

    lax.fori_loop(1, N_TP, sums, 0)

    sems = (send, recv, pr)
    ring_d = Ring(0, dbuf, 0, FAR_ROWS, sems, here)
    ring_c = [Ring(1, cbuf, 0, CSPLIT, sems, here), Ring(2, cbuf, CSPLIT, CBROWS - CSPLIT, sems, here)]
    ring_h = [Ring(3 + g, hbuf, a, n, sems, here) for g, (a, n) in enumerate(GROUPS)]

    passed = []
    landed = []

    def take_near(q):
        first = max(CAP, q * QROWS)
        rows = pl.ds(first, (q + 1) * QROWS - first)
        copy = remote(wide.at[rows], nbuf.at[core, rows], near_s.at[q], near_r.at[q], ep, here["next"])
        copy.wait_recv()
        landed.append(copy)
        rows = pl.ds(q * QROWS, QROWS)
        copy = remote(
            nbuf.at[core, rows], nbuf.at[core, rows], near_s.at[NEAR + q], near_r.at[NEAR + q], ep, here["partner"]
        )
        copy.start()
        passed.append(copy)

    def near_from_partner(q):
        rows = pl.ds(q * QROWS, QROWS)
        remote(
            nbuf.at[1 - core, rows], nbuf.at[1 - core, rows], near_s.at[NEAR + q], near_r.at[NEAR + q],
            ep, here["partner"],
        ).wait_recv()

    def hidden(q):
        if q < NEAR:
            near_from_partner(q)
            rows = slice(q * QROWS, (q + 1) * QROWS)
            a = dot(nbuf[0, rows, :], wg[:WIDE, :]) + dot(nbuf[1, rows, :], wg[WIDE:, :])
            b = dot(nbuf[0, rows, :], wu[:WIDE, :]) + dot(nbuf[1, rows, :], wu[WIDE:, :])
        else:
            rows = slice((q - NEAR) * QROWS, (q - NEAR + 1) * QROWS)
            lhs = jnp.concatenate([dbuf[t, rows, :] for t in range(N_TP)], axis=1)
            a, b = dot(lhs, wg[...]), dot(lhs, wu[...])
        hbuf[tp, q * QROWS : (q + 1) * QROWS, :] = (silu(a) * b).astype(BF16)

    def down(g, chip, first):
        a, n = GROUPS[g]
        rows = slice(a, a + n)
        lhs = jnp.concatenate([hbuf[chip * NC, rows, :], hbuf[chip * NC + 1, rows, :]], axis=1)
        depth = pl.ds(pl.multiple_of(chip * NC * HID, NC * HID), NC * HID)
        a = dot(lhs, wd[depth, :])
        if first:
            oacc[rows, :] = a
        else:
            oacc[rows, :] += a

    def returned(g):
        first, end = max(CAP, GROUPS[g][0]), sum(GROUPS[g])
        rows = pl.ds(first, end - first)
        return remote(outb.at[rows], rbuf.at[rows], back_s.at[g], back_r.at[g], ep, here["next"])

    def combine(g):
        returned(g).wait_recv()
        a, n = GROUPS[g]
        rows = slice(a, a + n)
        return dot(chi[rows, :], rbuf[rows, :], TN) + dot(clo[rows, :], rbuf[rows, :], TN)

    def give_back(g):
        a, n = GROUPS[g]
        outb[a : a + n, :] = oacc[a : a + n, :].astype(BF16)

        def back(r, carry):
            rows = pl.ds(r * CAP, CAP)
            remote(outb.at[rows], rbuf.at[rows], back_s.at[g], back_r.at[g], peer(r, -1), tp).start()
            return carry

        lax.fori_loop(max(1, a // CAP), (a + n) // CAP, back, 0)

    def h_down(g, d):
        if d in (1, 2, 3):
            down(g, ring_d.behind(d), False)
        if d > 0:
            ring_h[g].from_partner(d)
        down(g, ring_d.behind(-d), d == 0)

    def conv_down(part, d):
        if d > 0:
            ring_c[part].from_partner(d)
        rows = slice(part * CSPLIT, (part + 1) * CSPLIT)
        for sign in (-1, 1)[0 if 0 < d < 4 else 1 :]:
            chip = ring_d.chip(sign * d)
            depth = pl.ds(pl.multiple_of(chip * NC * CH, NC * CH), NC * CH)
            lhs = jnp.concatenate([cbuf[chip * NC, rows, :], cbuf[chip * NC + 1, rows, :]], axis=1)
            product = dot(lhs, wc[depth, :])
            if d == 0:
                filt[rows, :] = product
            else:
                filt[rows, :] += product

    take_near(0)
    dispatch_near(1)
    dispatch_near(2)
    loads[10].wait()
    loads[11].wait()
    hidden(0)
    ring_h[0].own()
    arrived = remote(packed, dbuf.at[tp], misc.at[0], misc.at[1], ep, here["next"])
    arrived.wait_recv()
    ring_d.own()
    ring_h[0].own2()
    rest = pl.ds(1, N_TP - 1)
    summed = remote(stat.at[rest], stat.at[rest], misc.at[4], misc.at[5], ep, here["next"])
    summed.wait_recv()
    total = stat[0]
    for r in range(1, N_TP):
        total = total + stat[r]
    total = total * (1.0 / D)
    mean, square = total[0:4, :], total[4:8, :]
    scale = lax.rsqrt(square - mean * mean + 1e-05)
    turned = jnp.concatenate([mean, scale], axis=0).T
    for r in range(4):
        part = filt[r * 128 : (r + 1) * 128, :]
        part = (part - turned[:, r : r + 1]) * turned[:, 4 + r : 5 + r]
        cbuf[tp, r * 128 : (r + 1) * 128, :] = silu(part * gain[...] + shift[...]).astype(BF16)
    ring_c[0].own()
    ring_d.own2()
    ring_c[0].own2()
    ring_h[0].stage(1)
    ring_d.stage(1)
    ring_c[0].stage(1)
    loads[13].wait()
    h_down(0, 0)
    take_near(1)
    take_near(2)
    pack(3)
    dispatch_near(3)
    pack(4)
    dispatch_near(4)
    ring_h[0].stage(2)
    hidden(1)
    hidden(2)
    ring_h[3].own()
    ring_d.stage(2)
    ring_c[0].stage(2)
    h_down(0, 1)
    ring_h[3].own2()
    ring_h[0].stage(3)
    ring_d.stage(3)
    ring_c[0].stage(3)
    ring_h[3].stage(1)
    h_down(0, 2)
    h_down(3, 0)
    ring_d.stage(4)
    ring_h[0].stage(4)
    ring_c[0].stage(4)
    ring_h[3].stage(2)
    for d in range(1, 5):
        ring_d.from_partner(d)
    hidden(5)
    hidden(6)
    hidden(7)
    ring_h[1].own()
    ring_h[1].own2()
    h_down(0, 3)
    h_down(0, 4)
    give_back(0)
    take_near(3)
    take_near(4)
    hidden(3)
    hidden(4)
    ring_h[2].own()
    ring_h[3].stage(3)
    ring_h[2].own2()
    h_down(3, 1)
    h_down(3, 2)
    ring_h[1].stage(1)
    ring_h[3].stage(4)
    ring_h[2].stage(1)
    h_down(3, 3)
    h_down(3, 4)
    give_back(3)
    h_down(1, 0)
    h_down(2, 0)
    ring_h[1].stage(2)
    ring_h[2].stage(2)
    ring_c[1].own()
    h_down(1, 1)
    h_down(2, 1)
    ring_c[1].own2()
    loads[12].wait()
    for d in range(5):
        conv_down(0, d)
    ring_h[1].stage(3)
    ring_h[2].stage(3)
    ring_c[1].stage(1)
    h_down(1, 2)
    h_down(2, 2)

    loads[14].wait()
    weight = jnp.zeros((N_EP, TOK), F32)
    for k in range(TOPK):
        weight = weight + jnp.where(routes[k : k + 1, :] == expert, rw[k : k + 1, :], 0.0)
    wslot[...] = weight
    for r in range(N_EP):
        w = wslot[r : r + 1, :]
        high = w.astype(BF16).astype(F32)
        hot = onehot[r * CAP : (r + 1) * CAP, :].astype(F32)
        chi[r * CAP : (r + 1) * CAP, :] = (hot * high).astype(BF16)
        clo[r * CAP : (r + 1) * CAP, :] = (hot * (w - high)).astype(BF16)
    h_down(1, 3)
    h_down(2, 3)
    ring_h[1].stage(4)
    ring_h[2].stage(4)
    h_down(1, 4)
    give_back(1)
    ring_c[1].stage(2)
    h_down(2, 4)
    give_back(2)
    ring_c[1].stage(3)
    for d in range(3):
        conv_down(1, d)
    loads[15].wait()

    rbuf[0:CAP, :] = outb[0:CAP, :]
    summed_up = combine(0) + combine(3)
    ring_c[1].stage(4)
    conv_down(1, 3)
    conv_down(1, 4)
    conv_o[...] = filt[...].astype(BF16)
    mid = jnp.concatenate([cbuf[t, ROWS_A:, :] for t in range(N_TP)], axis=0)
    summed_up = summed_up + dot(mid, sd[...], TN)
    moe_o[...] = (summed_up + combine(1) + combine(2)).astype(BF16)

    @pl.when(ep < N_EP - 1)
    def _():
        halo.wait_send()

    for copy in (arrived, summed, *[returned(g) for g in range(len(GROUPS))], *landed, *passed):
        copy.wait_send()
    for ring in (ring_d, *ring_c, *ring_h):
        ring.drain()


def body(*args):
    (
        conv_value, conv_gate, conv_taps, norm_gain, norm_shift, conv_out_weight, moe_input, moe_gain, routes,
        route_weights, expert_gate, expert_up, expert_down, shared_gate, shared_up, shared_down,
    ) = args
    operands = (
        conv_value, conv_gate, conv_taps, norm_gain.reshape(1, CH), norm_shift.reshape(1, CH), conv_out_weight,
        moe_input, moe_gain.reshape(1, D), routes.T, route_weights.T, expert_gate[0], expert_up[0], expert_down[0],
        shared_gate.T, shared_up.T, shared_down,
    )
    vmem = pltpu.VMEM
    dma = pltpu.SemaphoreType.DMA
    rings = 3 + len(GROUPS)
    outs = (vmem((ROWS_A, CH), BF16), vmem((TOK, CH), BF16))
    return pl.pallas_call(
        kernel,
        out_shape=outs,
        in_specs=[pl.BlockSpec(memory_space=pltpu.HBM)] * len(operands),
        out_specs=(pl.BlockSpec(memory_space=pltpu.VMEM),) * 2,
        scratch_shapes=[vmem(o.shape, o.dtype) for o in operands]
        + [
            vmem((HALO + ROWS_A, CH), F32),
            vmem((HALO, CH), BF16),
            vmem((HALO, CH), BF16),
            vmem((ROWS_A, CH), F32),
            vmem((N_TP, 8, CH), F32),
            vmem((TOK, D), BF16),
            vmem((N_EP, TOK), F32),
            vmem((N_EP, TOK), F32),
            vmem((SLOTS, TOK), BF16),
            vmem((NEAR_ROWS, WIDE), BF16),
            vmem((FAR_ROWS, CH), BF16),
            vmem((SLOTS, TOK), BF16),
            vmem((SLOTS, TOK), BF16),
            vmem((NC, NEAR_ROWS, WIDE), BF16),
            vmem((N_TP, FAR_ROWS, CH), BF16),
            vmem((N_TP, SLOTS, HID), BF16),
            vmem((N_TP, CBROWS, CH), BF16),
            vmem((SLOTS, CH), F32),
            vmem((SLOTS, CH), BF16),
            vmem((SLOTS, CH), BF16),
            dma((16,)),
            dma((6,)),
            dma((2 * NEAR,)),
            dma((2 * NEAR,)),
            dma((len(GROUPS),)),
            dma((len(GROUPS),)),
            dma((rings,)),
            dma((rings, 8)),
            dma((rings, 5)),
        ],
        compiler_params=pltpu.CompilerParams(
            collective_id=0, has_side_effects=True, vmem_limit_bytes=55 * 1024 * 1024
        ),
        cost_estimate=pl.CostEstimate(flops=5_000_000_000, bytes_accessed=8_000_000, transcendentals=0),
    )(*operands)


def solution(mesh):
    in_specs = (
        P("ep", "tp"),
        P("ep", "tp"),
        P(None, "tp"),
        P("tp"),
        P("tp"),
        P(None, "tp"),
        P("ep", None),
        P(),
        P("ep", None),
        P("ep", None),
        P("ep", None, "tp"),
        P("ep", None, "tp"),
        P("ep", None, "tp"),
        P(None, "tp"),
        P(None, "tp"),
        P(None, "tp"),
    )
    out_specs = (P("ep", "tp"), P("ep", "tp"))
    return jax.shard_map(body, mesh=mesh, in_specs=in_specs, out_specs=out_specs, check_vma=False)
```

```python
import functools

import jax
import jax.numpy as jnp
from jax import lax
from jax.experimental import pallas as pl
from jax.experimental.pallas import tpu as pltpu
from jax.sharding import PartitionSpec as P

MESH = pl.DeviceIdType.MESH
F32 = jnp.float32
BF16 = jnp.bfloat16

NZ, NX, NY, NC = 8, 4, 8, 2
N_EP, N_TP = NZ * NX, NY * NC
D = 2048
CH = D // N_TP
TAPS = 31
HALO = 32
ROWS_A = 512
TOK = 128
CAP = 32
SLOTS = N_EP * CAP
TOPK = 4
HID = 256
SH = 32
QROWS = NX * CAP
NEAR = 5
NEAR_BLOCKS = NEAR * NX
NEAR_ROWS = NEAR * QROWS
FAR_ROWS = SLOTS - NEAR_ROWS
WIDE = D // NC
GROUPS = ((0, 128), (640, 384), (384, 256), (128, 256))
CBROWS = ROWS_A + SH
CSPLIT = 128


def dot(a, b, dims=(((1,), (0,)), ((), ())), precision=None):
    return lax.dot_general(a, b, dims, precision=precision, preferred_element_type=F32)


NT = (((1,), (1,)), ((), ()))
TN = (((0,), (0,)), ((), ()))


def sigmoid(v):
    return 1.0 / (1.0 + jnp.exp(-v))


def silu(v):
    return v / (1.0 + jnp.exp(-v))


class Ring:
    def __init__(self, place, buffer, first, rows, sems, here):
        self.buffer, self.first, self.rows, self.here = buffer, first, rows, here
        send, recv, pr = sems
        self.send, self.recv, self.pr = send.at[place], recv.at[place], pr.at[place]

    def chip(self, d):
        return lax.rem(self.here["y"] + d + 2 * NY, NY)

    def behind(self, d):
        return lax.rem(self.here["y"] - self.here["way"] * d + 2 * NY, NY)

    def remote(self, ref, recv, to):
        return pltpu.make_async_remote_copy(
            src_ref=ref, dst_ref=ref, send_sem=self.send, recv_sem=recv,
            device_id=(self.here["ep"], to), device_id_type=MESH,
        )

    def at(self, chip, core, halved=False):
        if not halved:
            return self.buffer.at[chip * NC + core, pl.ds(self.first, self.rows)]
        half = self.rows // 2
        first = pl.multiple_of(self.first + self.here["core"] * half, 16)
        return self.buffer.at[chip * NC + core, pl.ds(first, half)]

    def many(self, n):
        return self.buffer.at[pl.ds(0, n), pl.ds(self.first, self.rows)]

    def own(self):
        h = self.here
        mine = self.at(h["y"], h["core"])
        self.remote(mine, self.pr.at[0], h["partner"]).start()
        self.remote(mine, self.recv.at[0], h["next"]).start()

    def own2(self):
        h = self.here
        other = self.at(h["y"], 1 - h["core"])
        self.remote(other, self.pr.at[0], h["partner"]).wait_recv()
        self.remote(other, self.recv.at[1], h["next"]).start()

    def stage(self, d):
        h = self.here
        chip = self.behind(d)
        for j, core in enumerate((h["core"], 1 - h["core"])):
            got = self.at(chip, core, d == 4)
            self.remote(got, self.recv.at[2 * d - 2 + j], h["next"]).wait_recv()
            if d < 4:
                self.remote(self.at(chip, core, d == 3), self.recv.at[2 * d + j], h["next"]).start()
            self.remote(got, self.pr.at[d], h["partner"]).start()

    def from_partner(self, d):
        got = self.many(2 if d < 4 else 1)
        self.remote(got, self.pr.at[d], self.here["partner"]).wait_recv()

    def drain(self):
        self.remote(self.many(N_TP - 1), self.pr.at[0], self.here["partner"]).wait_send()


def kernel(
    value_h, gate_h, taps_h, gain_h, shift_h, wc_h, x_h, mgain_h, routes_h, rw_h, wg_h, wu_h, wd_h, sg_h, su_h, sd_h,
    conv_o, moe_o,
    value, gate, taps, gain, shift, wc, x, mgain, routes, rw, wg, wu, wd, sg, su, sd,
    pad, halo_out, halo_in, filt, stat, normed, slot, wslot, onehot, wide, packed, chi, clo,
    nbuf, dbuf, hbuf, cbuf, oacc, outb, rbuf,
    load, misc, near_s, near_r, back_s, back_r, send, recv, pr,
):
    ep, tp = lax.axis_index("ep"), lax.axis_index("tp")
    z, xx = lax.div(ep, NX), lax.rem(ep, NX)
    y, core = lax.div(tp, NC), lax.rem(tp, NC)
    here = {
        "ep": ep, "y": y, "core": core,
        "way": 1 - 2 * core,
        "next": lax.rem(y + 1 - 2 * core + NY, NY) * NC + core,
        "partner": y * NC + (1 - core),
    }

    z_at = [lax.rem(z + d, NZ) * NX for d in range(NZ)]
    x_at = [lax.rem(xx + d, NX) for d in range(NX)]
    y_at = [lax.rem(y + d, NY) * NC for d in range(NY)]
    core_at = [core, 1 - core]

    def peer(rho, sign):
        q, dx = divmod(rho, NX)
        dz = (q + 1) // 2 if q % 2 else (NZ - q // 2) % NZ
        return z_at[sign * dz % NZ] + x_at[sign * dx % NX]

    def tp_peer(r):
        return y_at[r // NC] + core_at[r % NC]

    def remote(src, dst, send, recv, to_ep, to_tp):
        return pltpu.make_async_remote_copy(
            src_ref=src, dst_ref=dst, send_sem=send, recv_sem=recv, device_id=(to_ep, to_tp), device_id_type=MESH
        )

    loads = [
        pltpu.make_async_copy(a, b, load.at[i])
        for i, (a, b) in enumerate(
            (
                (x_h, x), (mgain_h, mgain), (routes_h, routes), (value_h, value), (gate_h, gate), (taps_h, taps),
                (gain_h, gain), (shift_h, shift), (sg_h, sg), (su_h, su), (wg_h, wg), (wu_h, wu), (wc_h, wc),
                (wd_h, wd), (rw_h, rw), (sd_h, sd),
            )
        )
    ]
    for i in (2, 3, 4, 1, 0):
        loads[i].start()

    barrier = pltpu.get_barrier_semaphore()

    for r in range(N_EP - 1, 0, -1):
        pl.semaphore_signal(barrier, inc=1, device_id=(peer(r, 1), tp), device_id_type=MESH)
    for r in range(N_TP - 1, 0, -1):
        pl.semaphore_signal(barrier, inc=1, device_id=(ep, tp_peer(r)), device_id_type=MESH)

    loads[2].wait()
    rho = lax.broadcasted_iota(jnp.int32, (N_EP, TOK), 0)
    q, dx = rho >> 2, rho & 3
    dz = jnp.where((q & 1) == 1, (q + 1) >> 1, (NZ - (q >> 1)) & 7)
    expert = ((z + dz) & 7) * NX + ((xx + dx) & 3)
    hits = jnp.zeros((N_EP, TOK), F32)
    for k in range(TOPK):
        hits = hits + jnp.where(routes[k : k + 1, :] == expert, 1.0, 0.0)
    before = jnp.where(
        lax.broadcasted_iota(jnp.int32, (TOK, TOK), 0) < lax.broadcasted_iota(jnp.int32, (TOK, TOK), 1), 1.0, 0.0
    ).astype(BF16)
    rank = dot(hits.astype(BF16), before)
    slot[...] = jnp.where(hits > 0.5, rank, -1.0)
    place = lax.broadcasted_iota(jnp.int32, (CAP, TOK), 0).astype(F32)
    for r in range(N_EP):
        onehot[r * CAP : (r + 1) * CAP, :] = jnp.where(slot[r : r + 1, :] == place, 1.0, 0.0).astype(BF16)


    loads[3].wait()
    loads[4].wait()
    glu = (value[...].astype(F32) * sigmoid(gate[...].astype(F32))).astype(BF16)
    pad[HALO:, :] = glu.astype(F32)
    halo_out[...] = glu[ROWS_A - HALO :, :]
    halo = remote(halo_out, halo_in, misc.at[2], misc.at[3], lax.rem(ep + 1, N_EP), tp)

    loads[1].wait()
    loads[0].wait()
    for r in range(0, TOK, 32):
        rows = x[r : r + 32, :].astype(F32)
        mean = jnp.mean(rows * rows, axis=1, keepdims=True)
        normed[r : r + 32, :] = (rows * lax.rsqrt(mean + 1e-06) * mgain[...]).astype(BF16)

    def pack(q):
        rows = slice(q * QROWS, (q + 1) * QROWS)
        mine = normed[:, pl.ds(pl.multiple_of(core * WIDE, WIDE), WIDE)]
        wide[rows, :] = dot(onehot[rows, :], mine).astype(BF16)

    pack(0)
    packed[...] = dot(onehot[NEAR_ROWS:, :], normed[:, pl.ds(pl.multiple_of(tp * CH, CH), CH)]).astype(BF16)

    pl.semaphore_wait(barrier, N_TP - 1 + N_EP - 1)

    def dispatch_far():
        for r in range(N_EP - 1, NEAR_BLOCKS - 1, -1):
            rows = pl.ds((r - NEAR_BLOCKS) * CAP, CAP)
            remote(packed.at[rows], dbuf.at[tp, rows], misc.at[0], misc.at[1], peer(r, 1), tp).start()

    def dispatch_near(q):
        for r in range(max(1, q * NX), (q + 1) * NX):
            rows = pl.ds(r * CAP, CAP)
            remote(wide.at[rows], nbuf.at[core, rows], near_s.at[0], near_r.at[q], peer(r, 1), tp).start()

    @pl.when(ep < N_EP - 1)
    def _():
        halo.start()

    dispatch_far()
    dispatch_near(0)
    for copy in loads[5:]:
        copy.start()
    nbuf[core, 0:CAP, :] = wide[0:CAP, :]
    for q in (1, 2):
        pack(q)

    loads[8].wait()
    loads[9].wait()
    shared = silu(dot(sg[...], normed[...], NT)) * dot(su[...], normed[...], NT)
    cbuf[tp, ROWS_A:, :] = shared.astype(BF16)

    loads[5].wait()
    loads[6].wait()
    loads[7].wait()
    pad[:HALO, :] = jnp.zeros((HALO, CH), F32)

    @pl.when(ep > 0)
    def _():
        halo.wait_recv()
        pad[:HALO, :] = halo_in[...].astype(F32)

    for b in range(0, ROWS_A, 64):
        total = jnp.zeros((64, CH), F32)
        for j in range(TAPS):
            first = b + j + HALO - (TAPS - 1)
            total = total + taps[j : j + 1, :] * pad[first : first + 64, :]
        filt[b : b + 64, :] = total
    ones = jnp.ones((8, CH), F32)
    for r in range(4):
        part = filt[r * 128 : (r + 1) * 128, :]
        stat[0, r : r + 1, :] = dot(ones, part, NT, lax.Precision.HIGHEST)[0:1, :]
        stat[0, 4 + r : 5 + r, :] = dot(ones, part * part, NT, lax.Precision.HIGHEST)[0:1, :]

    for r in range(N_TP - 1, 0, -1):
        remote(stat.at[0], stat.at[r], misc.at[4], misc.at[5], ep, tp_peer(r)).start()

    sems = (send, recv, pr)
    ring_d = Ring(0, dbuf, 0, FAR_ROWS, sems, here)
    ring_c = [Ring(1, cbuf, 0, CSPLIT, sems, here), Ring(2, cbuf, CSPLIT, CBROWS - CSPLIT, sems, here)]
    ring_h = [Ring(3 + g, hbuf, a, n, sems, here) for g, (a, n) in enumerate(GROUPS)]

    def take_near(q):
        first = max(CAP, q * QROWS)
        rows = pl.ds(first, (q + 1) * QROWS - first)
        remote(wide.at[rows], nbuf.at[core, rows], near_s.at[0], near_r.at[q], ep, here["next"]).wait_recv()
        rows = pl.ds(q * QROWS, QROWS)
        remote(
            nbuf.at[core, rows], nbuf.at[core, rows], near_s.at[1], near_r.at[NEAR + q], ep, here["partner"]
        ).start()

    def near_from_partner(q):
        rows = pl.ds(q * QROWS, QROWS)
        remote(
            nbuf.at[1 - core, rows], nbuf.at[1 - core, rows], near_s.at[1], near_r.at[NEAR + q],
            ep, here["partner"],
        ).wait_recv()

    def hidden(q):
        if q < NEAR:
            near_from_partner(q)
            rows = slice(q * QROWS, (q + 1) * QROWS)
            a = dot(nbuf[0, rows, :], wg[:WIDE, :]) + dot(nbuf[1, rows, :], wg[WIDE:, :])
            b = dot(nbuf[0, rows, :], wu[:WIDE, :]) + dot(nbuf[1, rows, :], wu[WIDE:, :])
        else:
            rows = slice((q - NEAR) * QROWS, (q - NEAR + 1) * QROWS)
            lhs = jnp.concatenate([dbuf[t, rows, :] for t in range(N_TP)], axis=1)
            a, b = dot(lhs, wg[...]), dot(lhs, wu[...])
        hbuf[tp, q * QROWS : (q + 1) * QROWS, :] = (silu(a) * b).astype(BF16)

    def down(g, chip, first):
        a, n = GROUPS[g]
        rows = slice(a, a + n)
        lhs = jnp.concatenate([hbuf[chip * NC, rows, :], hbuf[chip * NC + 1, rows, :]], axis=1)
        depth = pl.ds(pl.multiple_of(chip * NC * HID, NC * HID), NC * HID)
        a = dot(lhs, wd[depth, :])
        if first:
            oacc[rows, :] = a
        else:
            oacc[rows, :] += a

    def returned(g):
        first, end = max(CAP, GROUPS[g][0]), sum(GROUPS[g])
        rows = pl.ds(first, end - first)
        return remote(outb.at[rows], rbuf.at[rows], back_s.at[0], back_r.at[g], ep, here["next"])

    def combine(g):
        returned(g).wait_recv()
        a, n = GROUPS[g]
        rows = slice(a, a + n)
        return dot(chi[rows, :], rbuf[rows, :], TN) + dot(clo[rows, :], rbuf[rows, :], TN)

    def give_back(g):
        a, n = GROUPS[g]
        outb[a : a + n, :] = oacc[a : a + n, :].astype(BF16)

        for r in range(max(1, a // CAP), (a + n) // CAP):
            rows = pl.ds(r * CAP, CAP)
            remote(outb.at[rows], rbuf.at[rows], back_s.at[0], back_r.at[g], peer(r, -1), tp).start()

    def h_down(g, d):
        if d in (1, 2, 3):
            down(g, ring_d.behind(d), False)
        if d > 0:
            ring_h[g].from_partner(d)
        down(g, ring_d.behind(-d), d == 0)

    def conv_down(part, d):
        if d > 0:
            ring_c[part].from_partner(d)
        rows = slice(part * CSPLIT, (CSPLIT, ROWS_A)[part])
        for sign in (-1, 1)[0 if 0 < d < 4 else 1 :]:
            chip = ring_d.chip(sign * d)
            depth = pl.ds(pl.multiple_of(chip * NC * CH, NC * CH), NC * CH)
            lhs = jnp.concatenate([cbuf[chip * NC, rows, :], cbuf[chip * NC + 1, rows, :]], axis=1)
            product = dot(lhs, wc[depth, :])
            if d == 0:
                filt[rows, :] = product
            else:
                filt[rows, :] += product

    take_near(0)
    dispatch_near(1)
    dispatch_near(2)
    loads[10].wait()
    loads[11].wait()
    hidden(0)
    ring_h[0].own()
    arrived = remote(packed, dbuf.at[tp], misc.at[0], misc.at[1], ep, here["next"])
    arrived.wait_recv()
    ring_d.own()
    ring_h[0].own2()
    rest = pl.ds(1, N_TP - 1)
    summed = remote(stat.at[rest], stat.at[rest], misc.at[4], misc.at[5], ep, here["next"])
    summed.wait_recv()
    total = stat[0]
    for r in range(1, N_TP):
        total = total + stat[r]
    total = total * (1.0 / D)
    mean, square = total[0:4, :], total[4:8, :]
    scale = lax.rsqrt(square - mean * mean + 1e-05)
    turned = jnp.concatenate([mean, scale], axis=0).T
    for r in range(4):
        part = filt[r * 128 : (r + 1) * 128, :]
        part = (part - turned[:, r : r + 1]) * turned[:, 4 + r : 5 + r]
        cbuf[tp, r * 128 : (r + 1) * 128, :] = silu(part * gain[...] + shift[...]).astype(BF16)
    ring_c[0].own()
    ring_d.own2()
    ring_c[0].own2()
    ring_h[0].stage(1)
    ring_d.stage(1)
    ring_c[0].stage(1)
    loads[13].wait()
    h_down(0, 0)
    take_near(1)
    take_near(2)
    pack(3)
    dispatch_near(3)
    pack(4)
    dispatch_near(4)
    ring_h[0].stage(2)
    ring_d.stage(2)
    ring_c[0].stage(2)
    hidden(1)
    hidden(2)
    ring_h[3].own()
    h_down(0, 1)
    ring_h[3].own2()
    ring_h[0].stage(3)
    ring_d.stage(3)
    ring_c[0].stage(3)
    ring_h[3].stage(1)
    h_down(0, 2)
    h_down(3, 0)
    ring_d.stage(4)
    ring_h[0].stage(4)
    ring_c[0].stage(4)
    ring_h[3].stage(2)
    for d in range(1, 5):
        ring_d.from_partner(d)
    hidden(5)
    hidden(6)
    hidden(7)
    ring_h[1].own()
    ring_h[1].own2()
    h_down(0, 3)
    h_down(0, 4)
    give_back(0)
    take_near(3)
    take_near(4)
    hidden(3)
    hidden(4)
    ring_h[2].own()
    ring_h[3].stage(3)
    ring_h[2].own2()
    h_down(3, 1)
    h_down(3, 2)
    ring_h[1].stage(1)
    ring_h[3].stage(4)
    ring_h[2].stage(1)
    h_down(3, 3)
    h_down(3, 4)
    give_back(3)
    h_down(1, 0)
    h_down(2, 0)
    ring_h[1].stage(2)
    ring_h[2].stage(2)
    ring_c[1].own()
    h_down(1, 1)
    h_down(2, 1)
    ring_c[1].own2()
    loads[12].wait()
    for d in range(5):
        conv_down(0, d)
    ring_h[1].stage(3)
    ring_h[2].stage(3)
    ring_c[1].stage(1)
    h_down(1, 2)
    h_down(2, 2)

    loads[14].wait()
    weight = jnp.zeros((N_EP, TOK), F32)
    for k in range(TOPK):
        weight = weight + jnp.where(routes[k : k + 1, :] == expert, rw[k : k + 1, :], 0.0)
    wslot[...] = weight
    for r in range(N_EP):
        w = wslot[r : r + 1, :]
        high = w.astype(BF16).astype(F32)
        hot = onehot[r * CAP : (r + 1) * CAP, :].astype(F32)
        chi[r * CAP : (r + 1) * CAP, :] = (hot * high).astype(BF16)
        clo[r * CAP : (r + 1) * CAP, :] = (hot * (w - high)).astype(BF16)
    h_down(1, 3)
    h_down(2, 3)
    ring_h[1].stage(4)
    ring_h[2].stage(4)
    h_down(1, 4)
    give_back(1)
    ring_c[1].stage(2)
    h_down(2, 4)
    give_back(2)
    ring_c[1].stage(3)
    for d in range(3):
        conv_down(1, d)
    loads[15].wait()

    rbuf[0:CAP, :] = outb[0:CAP, :]
    summed_up = combine(0) + combine(3)
    ring_c[1].stage(4)
    conv_down(1, 3)
    conv_down(1, 4)
    conv_o[...] = filt[...].astype(BF16)
    mid = jnp.concatenate([cbuf[t, ROWS_A:, :] for t in range(N_TP)], axis=0)
    summed_up = summed_up + dot(mid, sd[...], TN)
    moe_o[...] = (summed_up + combine(1) + combine(2)).astype(BF16)

    @pl.when(ep < N_EP - 1)
    def _():
        halo.wait_send()

    rest = pl.ds(CAP, NEAR_ROWS - CAP)
    landed = remote(wide.at[rest], nbuf.at[core, rest], near_s.at[0], near_r.at[0], ep, here["next"])
    passed = remote(nbuf.at[core], nbuf.at[core], near_s.at[1], near_r.at[NEAR], ep, here["partner"])
    rest = pl.ds(CAP, SLOTS - CAP)
    returning = remote(outb.at[rest], rbuf.at[rest], back_s.at[0], back_r.at[0], ep, here["next"])
    for copy in (arrived, summed, landed, passed, returning):
        copy.wait_send()
    for ring in (ring_d, *ring_c, *ring_h):
        ring.drain()


def body(*args):
    (
        conv_value, conv_gate, conv_taps, norm_gain, norm_shift, conv_out_weight, moe_input, moe_gain, routes,
        route_weights, expert_gate, expert_up, expert_down, shared_gate, shared_up, shared_down,
    ) = args
    operands = (
        conv_value, conv_gate, conv_taps, norm_gain.reshape(1, CH), norm_shift.reshape(1, CH), conv_out_weight,
        moe_input, moe_gain.reshape(1, D), routes.T, route_weights.T, expert_gate[0], expert_up[0], expert_down[0],
        shared_gate.T, shared_up.T, shared_down,
    )
    vmem = pltpu.VMEM
    dma = pltpu.SemaphoreType.DMA
    rings = 3 + len(GROUPS)
    outs = (vmem((ROWS_A, CH), BF16), vmem((TOK, CH), BF16))
    return pl.pallas_call(
        kernel,
        out_shape=outs,
        in_specs=[pl.BlockSpec(memory_space=pltpu.HBM)] * len(operands),
        out_specs=(pl.BlockSpec(memory_space=pltpu.VMEM),) * 2,
        scratch_shapes=[vmem(o.shape, o.dtype) for o in operands]
        + [
            vmem((HALO + ROWS_A, CH), F32),
            vmem((HALO, CH), BF16),
            vmem((HALO, CH), BF16),
            vmem((ROWS_A, CH), F32),
            vmem((N_TP, 8, CH), F32),
            vmem((TOK, D), BF16),
            vmem((N_EP, TOK), F32),
            vmem((N_EP, TOK), F32),
            vmem((SLOTS, TOK), BF16),
            vmem((NEAR_ROWS, WIDE), BF16),
            vmem((FAR_ROWS, CH), BF16),
            vmem((SLOTS, TOK), BF16),
            vmem((SLOTS, TOK), BF16),
            vmem((NC, NEAR_ROWS, WIDE), BF16),
            vmem((N_TP, FAR_ROWS, CH), BF16),
            vmem((N_TP, SLOTS, HID), BF16),
            vmem((N_TP, CBROWS, CH), BF16),
            vmem((SLOTS, CH), F32),
            vmem((SLOTS, CH), BF16),
            vmem((SLOTS, CH), BF16),
            dma((16,)),
            dma((6,)),
            dma((2,)),
            dma((2 * NEAR,)),
            dma((1,)),
            dma((len(GROUPS),)),
            dma((rings,)),
            dma((rings, 8)),
            dma((rings, 5)),
        ],
        compiler_params=pltpu.CompilerParams(
            collective_id=0, has_side_effects=True, vmem_limit_bytes=55 * 1024 * 1024
        ),
        cost_estimate=pl.CostEstimate(flops=5_000_000_000, bytes_accessed=8_000_000, transcendentals=0),
    )(*operands)


def solution(mesh):
    in_specs = (
        P("ep", "tp"),
        P("ep", "tp"),
        P(None, "tp"),
        P("tp"),
        P("tp"),
        P(None, "tp"),
        P("ep", None),
        P(),
        P("ep", None),
        P("ep", None),
        P("ep", None, "tp"),
        P("ep", None, "tp"),
        P("ep", None, "tp"),
        P(None, "tp"),
        P(None, "tp"),
        P(None, "tp"),
    )
    out_specs = (P("ep", "tp"), P("ep", "tp"))
    return jax.shard_map(body, mesh=mesh, in_specs=in_specs, out_specs=out_specs, check_vma=False)
```

```python
import functools

import jax
import jax.numpy as jnp
from jax import lax
from jax.experimental import pallas as pl
from jax.experimental.pallas import tpu as pltpu
from jax.sharding import PartitionSpec as P

MESH = pl.DeviceIdType.MESH
F32 = jnp.float32
BF16 = jnp.bfloat16

NZ, NX, NY, NC = 8, 4, 8, 2
N_EP, N_TP = NZ * NX, NY * NC
D = 2048
CH = D // N_TP
TAPS = 31
HALO = 32
ROWS_A = 512
TOK = 128
CAP = 32
SLOTS = N_EP * CAP
TOPK = 4
HID = 256
SH = 32
QROWS = NX * CAP
NEAR = 5
NEAR_BLOCKS = NEAR * NX
NEAR_ROWS = NEAR * QROWS
FAR_ROWS = SLOTS - NEAR_ROWS
WIDE = D // NC
GROUPS = ((0, 128), (640, 384), (384, 256), (128, 256))
CBROWS = ROWS_A + SH
CSPLIT = 128


def dot(a, b, dims=(((1,), (0,)), ((), ())), precision=None):
    return lax.dot_general(a, b, dims, precision=precision, preferred_element_type=F32)


NT = (((1,), (1,)), ((), ()))
TN = (((0,), (0,)), ((), ()))


def sigmoid(v):
    return 1.0 / (1.0 + jnp.exp(-v))


def silu(v):
    return v / (1.0 + jnp.exp(-v))


class Ring:
    def __init__(self, place, buffer, first, rows, sems, here):
        self.buffer, self.first, self.rows, self.here = buffer, first, rows, here
        send, recv, pr = sems
        self.send, self.recv, self.pr = send.at[place], recv.at[place], pr.at[place]

    def chip(self, d):
        return lax.rem(self.here["y"] + d + 2 * NY, NY)

    def behind(self, d):
        return lax.rem(self.here["y"] - self.here["way"] * d + 2 * NY, NY)

    def remote(self, ref, recv, to):
        return pltpu.make_async_remote_copy(
            src_ref=ref, dst_ref=ref, send_sem=self.send, recv_sem=recv,
            device_id=(self.here["ep"], to), device_id_type=MESH,
        )

    def at(self, chip, core, halved=False):
        if not halved:
            return self.buffer.at[chip * NC + core, pl.ds(self.first, self.rows)]
        half = self.rows // 2
        first = pl.multiple_of(self.first + self.here["core"] * half, 16)
        return self.buffer.at[chip * NC + core, pl.ds(first, half)]

    def many(self, n):
        return self.buffer.at[pl.ds(0, n), pl.ds(self.first, self.rows)]

    def own(self):
        h = self.here
        mine = self.at(h["y"], h["core"])
        self.remote(mine, self.pr.at[0], h["partner"]).start()
        self.remote(mine, self.recv.at[0], h["next"]).start()

    def own2(self):
        h = self.here
        other = self.at(h["y"], 1 - h["core"])
        self.remote(other, self.pr.at[0], h["partner"]).wait_recv()
        self.remote(other, self.recv.at[1], h["next"]).start()

    def stage(self, d):
        h = self.here
        chip = self.behind(d)
        for j, core in enumerate((h["core"], 1 - h["core"])):
            got = self.at(chip, core, d == 4)
            self.remote(got, self.recv.at[2 * d - 2 + j], h["next"]).wait_recv()
            if d < 4:
                self.remote(self.at(chip, core, d == 3), self.recv.at[2 * d + j], h["next"]).start()
            self.remote(got, self.pr.at[d], h["partner"]).start()

    def from_partner(self, d):
        got = self.many(2 if d < 4 else 1)
        self.remote(got, self.pr.at[d], self.here["partner"]).wait_recv()

    def drain(self):
        self.remote(self.many(N_TP - 1), self.pr.at[0], self.here["partner"]).wait_send()


def kernel(
    value_h, gate_h, taps_h, gain_h, shift_h, wc_h, x_h, mgain_h, routes_h, rw_h, wg_h, wu_h, wd_h, sg_h, su_h, sd_h,
    conv_o, moe_o,
    value, gate, taps, gain, shift, wc, x, mgain, routes, rw, wg, wu, wd, sg, su, sd,
    pad, halo_out, halo_in, filt, stat, normed, slot, wslot, onehot, wide, packed, chi, clo, high_t, low_t,
    nbuf, dbuf, hbuf, cbuf, oacc, outb, rbuf,
    load, misc, near_s, near_r, back_s, back_r, send, recv, pr,
):
    ep, tp = lax.axis_index("ep"), lax.axis_index("tp")
    z, xx = lax.div(ep, NX), lax.rem(ep, NX)
    y, core = lax.div(tp, NC), lax.rem(tp, NC)
    here = {
        "ep": ep, "y": y, "core": core,
        "way": 1 - 2 * core,
        "next": lax.rem(y + 1 - 2 * core + NY, NY) * NC + core,
        "partner": y * NC + (1 - core),
    }

    z_at = [lax.rem(z + d, NZ) * NX for d in range(NZ)]
    x_at = [lax.rem(xx + d, NX) for d in range(NX)]
    y_at = [lax.rem(y + d, NY) * NC for d in range(NY)]
    core_at = [core, 1 - core]

    def peer(rho, sign):
        q, dx = divmod(rho, NX)
        dz = (q + 1) // 2 if q % 2 else (NZ - q // 2) % NZ
        return z_at[sign * dz % NZ] + x_at[sign * dx % NX]

    def tp_peer(r):
        return y_at[r // NC] + core_at[r % NC]

    def remote(src, dst, send, recv, to_ep, to_tp):
        return pltpu.make_async_remote_copy(
            src_ref=src, dst_ref=dst, send_sem=send, recv_sem=recv, device_id=(to_ep, to_tp), device_id_type=MESH
        )

    loads = [
        pltpu.make_async_copy(a, b, load.at[i])
        for i, (a, b) in enumerate(
            (
                (x_h, x), (mgain_h, mgain), (routes_h, routes), (value_h, value), (gate_h, gate), (taps_h, taps),
                (gain_h, gain), (shift_h, shift), (sg_h, sg), (su_h, su), (wg_h, wg), (wu_h, wu), (wc_h, wc),
                (wd_h, wd), (rw_h, rw), (sd_h, sd),
            )
        )
    ]
    for i in (2, 3, 4, 1, 0):
        loads[i].start()

    barrier = pltpu.get_barrier_semaphore()

    for r in range(N_EP - 1, 0, -1):
        pl.semaphore_signal(barrier, inc=1, device_id=(peer(r, 1), tp), device_id_type=MESH)
    for r in range(N_TP - 1, 0, -1):
        pl.semaphore_signal(barrier, inc=1, device_id=(ep, tp_peer(r)), device_id_type=MESH)

    loads[2].wait()
    rho = lax.broadcasted_iota(jnp.int32, (N_EP, TOK), 0)
    q, dx = rho >> 2, rho & 3
    dz = jnp.where((q & 1) == 1, (q + 1) >> 1, (NZ - (q >> 1)) & 7)
    expert = ((z + dz) & 7) * NX + ((xx + dx) & 3)
    hits = jnp.zeros((N_EP, TOK), F32)
    for k in range(TOPK):
        hits = hits + jnp.where(routes[k : k + 1, :] == expert, 1.0, 0.0)
    before = jnp.where(
        lax.broadcasted_iota(jnp.int32, (TOK, TOK), 0) < lax.broadcasted_iota(jnp.int32, (TOK, TOK), 1), 1.0, 0.0
    ).astype(BF16)
    rank = dot(hits.astype(BF16), before)
    slot[...] = jnp.where(hits > 0.5, rank, -1.0)
    place = lax.broadcasted_iota(jnp.int32, (CAP, TOK), 0).astype(F32)
    for r in range(N_EP):
        onehot[r * CAP : (r + 1) * CAP, :] = jnp.where(slot[r : r + 1, :] == place, 1.0, 0.0).astype(BF16)


    loads[3].wait()
    loads[4].wait()
    glu = (value[...].astype(F32) * sigmoid(gate[...].astype(F32))).astype(BF16)
    pad[HALO:, :] = glu.astype(F32)
    halo_out[...] = glu[ROWS_A - HALO :, :]
    halo = remote(halo_out, halo_in, misc.at[2], misc.at[3], lax.rem(ep + 1, N_EP), tp)

    loads[1].wait()
    loads[0].wait()
    for r in range(0, TOK, 32):
        rows = x[r : r + 32, :].astype(F32)
        mean = jnp.mean(rows * rows, axis=1, keepdims=True)
        normed[r : r + 32, :] = (rows * lax.rsqrt(mean + 1e-06) * mgain[...]).astype(BF16)

    def pack(q):
        rows = slice(q * QROWS, (q + 1) * QROWS)
        mine = normed[:, pl.ds(pl.multiple_of(core * WIDE, WIDE), WIDE)]
        wide[rows, :] = dot(onehot[rows, :], mine).astype(BF16)

    pack(0)
    packed[...] = dot(onehot[NEAR_ROWS:, :], normed[:, pl.ds(pl.multiple_of(tp * CH, CH), CH)]).astype(BF16)

    pl.semaphore_wait(barrier, N_TP - 1 + N_EP - 1)

    def dispatch_far():
        for r in range(N_EP - 1, NEAR_BLOCKS - 1, -1):
            rows = pl.ds((r - NEAR_BLOCKS) * CAP, CAP)
            remote(packed.at[rows], dbuf.at[tp, rows], misc.at[0], misc.at[1], peer(r, 1), tp).start()

    def dispatch_near(q):
        for r in range(max(1, q * NX), (q + 1) * NX):
            rows = pl.ds(r * CAP, CAP)
            remote(wide.at[rows], nbuf.at[core, rows], near_s.at[0], near_r.at[q], peer(r, 1), tp).start()

    @pl.when(ep < N_EP - 1)
    def _():
        halo.start()

    dispatch_far()
    dispatch_near(0)
    for copy in loads[5:]:
        copy.start()
    nbuf[core, 0:CAP, :] = wide[0:CAP, :]
    for q in (1, 2):
        pack(q)

    loads[8].wait()
    loads[9].wait()
    shared = silu(dot(sg[...], normed[...], NT)) * dot(su[...], normed[...], NT)
    cbuf[tp, ROWS_A:, :] = shared.astype(BF16)

    loads[5].wait()
    loads[6].wait()
    loads[7].wait()
    pad[:HALO, :] = jnp.zeros((HALO, CH), F32)

    @pl.when(ep > 0)
    def _():
        halo.wait_recv()
        pad[:HALO, :] = halo_in[...].astype(F32)

    for b in range(0, ROWS_A, 64):
        total = jnp.zeros((64, CH), F32)
        for j in range(TAPS):
            first = b + j + HALO - (TAPS - 1)
            total = total + taps[j : j + 1, :] * pad[first : first + 64, :]
        filt[b : b + 64, :] = total
    ones = jnp.ones((8, CH), F32)
    for r in range(4):
        part = filt[r * 128 : (r + 1) * 128, :]
        stat[0, r : r + 1, :] = dot(ones, part, NT, lax.Precision.HIGHEST)[0:1, :]
        stat[0, 4 + r : 5 + r, :] = dot(ones, part * part, NT, lax.Precision.HIGHEST)[0:1, :]

    for r in range(N_TP - 1, 0, -1):
        remote(stat.at[0], stat.at[r], misc.at[4], misc.at[5], ep, tp_peer(r)).start()

    sems = (send, recv, pr)
    ring_d = Ring(0, dbuf, 0, FAR_ROWS, sems, here)
    ring_c = [Ring(1, cbuf, 0, CSPLIT, sems, here), Ring(2, cbuf, CSPLIT, CBROWS - CSPLIT, sems, here)]
    ring_h = [Ring(3 + g, hbuf, a, n, sems, here) for g, (a, n) in enumerate(GROUPS)]

    def take_near(q):
        first = max(CAP, q * QROWS)
        rows = pl.ds(first, (q + 1) * QROWS - first)
        remote(wide.at[rows], nbuf.at[core, rows], near_s.at[0], near_r.at[q], ep, here["next"]).wait_recv()
        rows = pl.ds(q * QROWS, QROWS)
        remote(
            nbuf.at[core, rows], nbuf.at[core, rows], near_s.at[1], near_r.at[NEAR + q], ep, here["partner"]
        ).start()

    def near_from_partner(q):
        rows = pl.ds(q * QROWS, QROWS)
        remote(
            nbuf.at[1 - core, rows], nbuf.at[1 - core, rows], near_s.at[1], near_r.at[NEAR + q],
            ep, here["partner"],
        ).wait_recv()

    def hidden(q):
        if q < NEAR:
            near_from_partner(q)
            rows = slice(q * QROWS, (q + 1) * QROWS)
            a = dot(nbuf[0, rows, :], wg[:WIDE, :]) + dot(nbuf[1, rows, :], wg[WIDE:, :])
            b = dot(nbuf[0, rows, :], wu[:WIDE, :]) + dot(nbuf[1, rows, :], wu[WIDE:, :])
        else:
            rows = slice((q - NEAR) * QROWS, (q - NEAR + 1) * QROWS)
            lhs = jnp.concatenate([dbuf[t, rows, :] for t in range(N_TP)], axis=1)
            a, b = dot(lhs, wg[...]), dot(lhs, wu[...])
        hbuf[tp, q * QROWS : (q + 1) * QROWS, :] = (silu(a) * b).astype(BF16)

    def down(g, chip, first):
        a, n = GROUPS[g]
        rows = slice(a, a + n)
        lhs = jnp.concatenate([hbuf[chip * NC, rows, :], hbuf[chip * NC + 1, rows, :]], axis=1)
        depth = pl.ds(pl.multiple_of(chip * NC * HID, NC * HID), NC * HID)
        a = dot(lhs, wd[depth, :])
        if first:
            oacc[rows, :] = a
        else:
            oacc[rows, :] += a

    def returned(g):
        first, end = max(CAP, GROUPS[g][0]), sum(GROUPS[g])
        rows = pl.ds(first, end - first)
        return remote(outb.at[rows], rbuf.at[rows], back_s.at[0], back_r.at[g], ep, here["next"])

    def combine(g):
        returned(g).wait_recv()
        a, n = GROUPS[g]
        rows = slice(a, a + n)
        return dot(high_t[:, rows], rbuf[rows, :]) + dot(low_t[:, rows], rbuf[rows, :])

    def give_back(g):
        a, n = GROUPS[g]
        outb[a : a + n, :] = oacc[a : a + n, :].astype(BF16)

        for r in range((a + n) // CAP - 1, max(1, a // CAP) - 1, -1):
            rows = pl.ds(r * CAP, CAP)
            remote(outb.at[rows], rbuf.at[rows], back_s.at[0], back_r.at[g], peer(r, -1), tp).start()

    def h_down(g, d):
        if d in (1, 2, 3):
            down(g, ring_d.behind(d), False)
        if d > 0:
            ring_h[g].from_partner(d)
        down(g, ring_d.behind(-d), d == 0)

    def conv_down(part, d):
        if d > 0:
            ring_c[part].from_partner(d)
        rows = slice(part * CSPLIT, (CSPLIT, ROWS_A)[part])
        for sign in (-1, 1)[0 if 0 < d < 4 else 1 :]:
            chip = ring_d.chip(sign * d)
            depth = pl.ds(pl.multiple_of(chip * NC * CH, NC * CH), NC * CH)
            lhs = jnp.concatenate([cbuf[chip * NC, rows, :], cbuf[chip * NC + 1, rows, :]], axis=1)
            product = dot(lhs, wc[depth, :])
            if d == 0:
                filt[rows, :] = product
            else:
                filt[rows, :] += product

    take_near(0)
    dispatch_near(1)
    dispatch_near(2)
    loads[10].wait()
    loads[11].wait()
    hidden(0)
    ring_h[0].own()
    arrived = remote(packed, dbuf.at[tp], misc.at[0], misc.at[1], ep, here["next"])
    arrived.wait_recv()
    ring_d.own()
    ring_h[0].own2()
    rest = pl.ds(1, N_TP - 1)
    summed = remote(stat.at[rest], stat.at[rest], misc.at[4], misc.at[5], ep, here["next"])
    summed.wait_recv()
    total = stat[0]
    for r in range(1, N_TP):
        total = total + stat[r]
    total = total * (1.0 / D)
    mean, square = total[0:4, :], total[4:8, :]
    scale = lax.rsqrt(square - mean * mean + 1e-05)
    turned = jnp.concatenate([mean, scale], axis=0).T
    for r in range(4):
        part = filt[r * 128 : (r + 1) * 128, :]
        part = (part - turned[:, r : r + 1]) * turned[:, 4 + r : 5 + r]
        cbuf[tp, r * 128 : (r + 1) * 128, :] = silu(part * gain[...] + shift[...]).astype(BF16)
    ring_c[0].own()
    ring_d.own2()
    ring_c[0].own2()
    ring_h[0].stage(1)
    ring_d.stage(1)
    ring_c[0].stage(1)
    loads[13].wait()
    h_down(0, 0)
    take_near(1)
    take_near(2)
    pack(3)
    dispatch_near(3)
    pack(4)
    dispatch_near(4)
    ring_h[0].stage(2)
    ring_d.stage(2)
    ring_c[0].stage(2)
    hidden(1)
    hidden(2)
    ring_h[3].own()
    h_down(0, 1)
    ring_h[3].own2()
    ring_h[0].stage(3)
    ring_d.stage(3)
    ring_c[0].stage(3)
    ring_h[3].stage(1)
    h_down(0, 2)
    h_down(3, 0)
    ring_d.stage(4)
    ring_h[0].stage(4)
    ring_c[0].stage(4)
    ring_h[3].stage(2)
    for d in range(1, 5):
        ring_d.from_partner(d)
    hidden(5)
    hidden(6)
    hidden(7)
    ring_h[1].own()
    ring_h[1].own2()
    h_down(0, 3)
    h_down(0, 4)
    give_back(0)
    take_near(3)
    take_near(4)
    hidden(3)
    hidden(4)
    ring_h[2].own()
    ring_h[3].stage(3)
    ring_h[2].own2()
    h_down(3, 1)
    h_down(3, 2)
    ring_h[1].stage(1)
    ring_h[3].stage(4)
    ring_h[2].stage(1)
    h_down(3, 3)
    h_down(3, 4)
    give_back(3)
    h_down(1, 0)
    h_down(2, 0)
    ring_h[1].stage(2)
    ring_h[2].stage(2)
    ring_c[1].own()
    h_down(1, 1)
    h_down(2, 1)
    ring_c[1].own2()
    loads[12].wait()
    for d in range(5):
        conv_down(0, d)
    ring_h[1].stage(3)
    ring_h[2].stage(3)
    ring_c[1].stage(1)
    h_down(1, 2)
    h_down(2, 2)

    loads[14].wait()
    weight = jnp.zeros((N_EP, TOK), F32)
    for k in range(TOPK):
        weight = weight + jnp.where(routes[k : k + 1, :] == expert, rw[k : k + 1, :], 0.0)
    wslot[...] = weight
    for r in range(N_EP):
        w = wslot[r : r + 1, :]
        high = w.astype(BF16).astype(F32)
        hot = onehot[r * CAP : (r + 1) * CAP, :].astype(F32)
        chi[r * CAP : (r + 1) * CAP, :] = (hot * high).astype(BF16)
        clo[r * CAP : (r + 1) * CAP, :] = (hot * (w - high)).astype(BF16)
    high_t[...] = chi[...].T
    low_t[...] = clo[...].T
    h_down(1, 3)
    h_down(2, 3)
    ring_h[1].stage(4)
    ring_h[2].stage(4)
    h_down(1, 4)
    give_back(1)
    ring_c[1].stage(2)
    h_down(2, 4)
    give_back(2)
    ring_c[1].stage(3)
    for d in range(3):
        conv_down(1, d)
    loads[15].wait()

    rbuf[0:CAP, :] = outb[0:CAP, :]
    summed_up = combine(0) + combine(3)
    ring_c[1].stage(4)
    conv_down(1, 3)
    conv_down(1, 4)
    conv_o[...] = filt[...].astype(BF16)
    mid = jnp.concatenate([cbuf[t, ROWS_A:, :] for t in range(N_TP)], axis=0)
    summed_up = summed_up + dot(mid, sd[...], TN)
    moe_o[...] = (summed_up + combine(1) + combine(2)).astype(BF16)

    @pl.when(ep < N_EP - 1)
    def _():
        halo.wait_send()

    rest = pl.ds(CAP, NEAR_ROWS - CAP)
    landed = remote(wide.at[rest], nbuf.at[core, rest], near_s.at[0], near_r.at[0], ep, here["next"])
    passed = remote(nbuf.at[core], nbuf.at[core], near_s.at[1], near_r.at[NEAR], ep, here["partner"])
    rest = pl.ds(CAP, SLOTS - CAP)
    returning = remote(outb.at[rest], rbuf.at[rest], back_s.at[0], back_r.at[0], ep, here["next"])
    for copy in (arrived, summed, landed, passed, returning):
        copy.wait_send()
    for ring in (ring_d, *ring_c, *ring_h):
        ring.drain()


def body(*args):
    (
        conv_value, conv_gate, conv_taps, norm_gain, norm_shift, conv_out_weight, moe_input, moe_gain, routes,
        route_weights, expert_gate, expert_up, expert_down, shared_gate, shared_up, shared_down,
    ) = args
    operands = (
        conv_value, conv_gate, conv_taps, norm_gain.reshape(1, CH), norm_shift.reshape(1, CH), conv_out_weight,
        moe_input, moe_gain.reshape(1, D), routes.T, route_weights.T, expert_gate[0], expert_up[0], expert_down[0],
        shared_gate.T, shared_up.T, shared_down,
    )
    vmem = pltpu.VMEM
    dma = pltpu.SemaphoreType.DMA
    rings = 3 + len(GROUPS)
    outs = (vmem((ROWS_A, CH), BF16), vmem((TOK, CH), BF16))
    return pl.pallas_call(
        kernel,
        out_shape=outs,
        in_specs=[pl.BlockSpec(memory_space=pltpu.HBM)] * len(operands),
        out_specs=(pl.BlockSpec(memory_space=pltpu.VMEM),) * 2,
        scratch_shapes=[vmem(o.shape, o.dtype) for o in operands]
        + [
            vmem((HALO + ROWS_A, CH), F32),
            vmem((HALO, CH), BF16),
            vmem((HALO, CH), BF16),
            vmem((ROWS_A, CH), F32),
            vmem((N_TP, 8, CH), F32),
            vmem((TOK, D), BF16),
            vmem((N_EP, TOK), F32),
            vmem((N_EP, TOK), F32),
            vmem((SLOTS, TOK), BF16),
            vmem((NEAR_ROWS, WIDE), BF16),
            vmem((FAR_ROWS, CH), BF16),
            vmem((SLOTS, TOK), BF16),
            vmem((SLOTS, TOK), BF16),
            vmem((TOK, SLOTS), BF16),
            vmem((TOK, SLOTS), BF16),
            vmem((NC, NEAR_ROWS, WIDE), BF16),
            vmem((N_TP, FAR_ROWS, CH), BF16),
            vmem((N_TP, SLOTS, HID), BF16),
            vmem((N_TP, CBROWS, CH), BF16),
            vmem((SLOTS, CH), F32),
            vmem((SLOTS, CH), BF16),
            vmem((SLOTS, CH), BF16),
            dma((16,)),
            dma((6,)),
            dma((2,)),
            dma((2 * NEAR,)),
            dma((1,)),
            dma((len(GROUPS),)),
            dma((rings,)),
            dma((rings, 8)),
            dma((rings, 5)),
        ],
        compiler_params=pltpu.CompilerParams(
            collective_id=0, has_side_effects=True, vmem_limit_bytes=55 * 1024 * 1024
        ),
        cost_estimate=pl.CostEstimate(flops=5_000_000_000, bytes_accessed=8_000_000, transcendentals=0),
    )(*operands)


def solution(mesh):
    in_specs = (
        P("ep", "tp"),
        P("ep", "tp"),
        P(None, "tp"),
        P("tp"),
        P("tp"),
        P(None, "tp"),
        P("ep", None),
        P(),
        P("ep", None),
        P("ep", None),
        P("ep", None, "tp"),
        P("ep", None, "tp"),
        P("ep", None, "tp"),
        P(None, "tp"),
        P(None, "tp"),
        P(None, "tp"),
    )
    out_specs = (P("ep", "tp"), P("ep", "tp"))
    return jax.shard_map(body, mesh=mesh, in_specs=in_specs, out_specs=out_specs, check_vma=False)
```
